256 devices in a mesh: fs: 32 (over z, y), tp: 8 (over x, core).
Axes of the slice: x: 4, y: 4, z: 8, core: 2. Of those that a mesh axis runs over, the one named last changes fastest.
Arguments:
- stream: bfloat16 [12288, 2048], P('fs', 'tp'), may hold values from -3 to 3
- gain_first: float32 [2048], replicated, may hold values from 0.1 to 1.9
- gain_mixer: float32 [2048], replicated, may hold values from 0.1 to 1.9
- gain_second: float32 [2048], replicated, may hold values from 0.1 to 1.9
- gate_weight: float32 [2048, 5632], P('fs', 'tp'), may hold values from -0.125 to 0.125
- gate_scale: float32 [5632], P('tp'), may hold values from 0.5 to 2
- up_weight: float32 [2048, 5632], P('fs', 'tp'), may hold values from -0.125 to 0.125
- up_scale: float32 [5632], P('tp'), may hold values from 0.5 to 2
- down_weight: float32 [5632, 2048], P('tp', 'fs'), may hold values from -0.15625 to 0.15625
- down_scale: float32 [2048], P('tp'), may hold values from 0.5 to 2
- pool_in_weight: float32 [2048, 512], P('fs', 'tp'), may hold values from -0.125 to 0.125
- pool_in_scale: float32 [512], P('tp'), may hold values from 0.5 to 2
- pool_out_weight: float32 [512, 2048], P('tp', 'fs'), may hold values from -0.5 to 0.5
- pool_out_scale: float32 [2048], P('tp'), may hold values from 0.5 to 2
Outputs:
- layer_out: bfloat16 [12288, 2048], P('fs', 'tp')
The draws below stay inside these ranges and needn't reach their ends.
All inputs are finite; a program needn't handle non-finite values.
Results may differ from the reference program's by a relative error of at most 0.025.
Values may be sent and summed in bfloat16 or wider, within the bound.
A program may use at most 64 MiB of HBM per device.

```python
import math
import jax
import jax.numpy as jnp
from jax import lax

D = 2048
FF = 5632
P_SIZE = 512
SEQ = 128
TOKENS = 12288
N_TP = 8


def strengthened(drawn, rng, source, target, blocks, factor):
    owner, partner = [(jnp.arange(drawn.shape[dim]) // (drawn.shape[dim] // blocks)).reshape([-1 if axis == dim else 1 for axis in range(drawn.ndim)]) for dim in (source, target)]
    chosen = jax.random.permutation(rng, blocks)[partner]
    strong = (owner == chosen) | (owner == (partner + blocks // 2) % blocks)
    return jnp.where(strong, factor * drawn, drawn)


def level_of(stream_key, extent, cuts, least, top_value):
    level, own = 1.0, jax.random.fold_in(stream_key, 6)
    for axis_at, blocks in cuts:
        steps = jnp.exp(jax.random.uniform(jax.random.fold_in(own, axis_at), (blocks,), jnp.float32, least / len(cuts), top_value / len(cuts)))
        level = level * jnp.repeat(steps, extent[axis_at] // blocks).reshape([-1 if axis == axis_at else 1 for axis in range(len(extent))])
    return level


def normal_values(own_key, extent, scale, limit, cuts=(), kind=jnp.bfloat16):
    values = jax.random.normal(own_key, extent, jnp.float32) * scale
    if len(cuts) > 0:
        values = level_of(own_key, extent, cuts, -0.22, 0.18) * values
    return jnp.clip(values, min=-limit, max=limit).astype(kind)


def heavy_noise(key, shape, width, bound, pieces, heavy, dtype=jnp.bfloat16):
    result = width * jax.random.normal(key, shape, jnp.float32)
    if pieces:
        result = result * level_of(key, shape, pieces, -0.22, 0.18)
    return jnp.clip(strengthened(result, jax.random.fold_in(key, 3), *heavy), -bound, bound).astype(dtype)


def setup_inputs(seed: int = 0) -> dict:
    streams_of = jax.random.split(jax.random.key(seed), 15)
    return {
        "stream": normal_values(streams_of[0], (TOKENS, D), 0.5, 3.0, ((0, 32), (1, 8))),
        "gain_first": jnp.clip(1.0 + 0.18 * jax.random.normal(streams_of[1], (D,), jnp.float32), 0.1, 1.9),
        "gain_mixer": jnp.clip(1.0 + 0.18 * jax.random.normal(streams_of[2], (D,), jnp.float32), 0.1, 1.9),
        "gain_second": jnp.clip(1.0 + 0.18 * jax.random.normal(streams_of[3], (D,), jnp.float32), 0.1, 1.9),
        "gate_weight": normal_values(streams_of[4], (D, FF), D ** -0.5, 0.125, ((0, 32), (1, 8)), jnp.float32),
        "gate_scale": jnp.clip(jnp.exp(math.log(2.0) - 1.3862944 * jax.random.uniform(streams_of[5], (FF,), jnp.float32) ** level_of(streams_of[5], (FF,), ((0, 8),), -0.2, 0.2)), 0.5, 2.0),
        "up_weight": normal_values(streams_of[6], (D, FF), D ** -0.5, 0.125, ((0, 32), (1, 8)), jnp.float32),
        "up_scale": jnp.clip(jnp.exp(math.log(2.0) - 1.3862944 * jax.random.uniform(streams_of[7], (FF,), jnp.float32) ** level_of(streams_of[7], (FF,), ((0, 8),), -0.2, 0.2)), 0.5, 2.0),
        "down_weight": heavy_noise(streams_of[8], (FF, D), FF ** -0.5, 0.15625, ((0, 8), (1, 32)), (0, 1, 32, 2.75), jnp.float32),
        "down_scale": jnp.clip(jnp.exp(math.log(2.0) - 1.3862944 * jax.random.uniform(streams_of[9], (D,), jnp.float32) ** level_of(streams_of[9], (D,), ((0, 8),), -0.2, 0.2)), 0.5, 2.0),
        "pool_in_weight": normal_values(streams_of[10], (D, P_SIZE), D ** -0.5, 0.125, ((0, 32), (1, 8)), jnp.float32),
        "pool_in_scale": jnp.clip(jnp.exp(math.log(2.0) - 1.3862944 * jax.random.uniform(streams_of[11], (P_SIZE,), jnp.float32) ** level_of(streams_of[11], (P_SIZE,), ((0, 8),), -0.2, 0.2)), 0.5, 2.0),
        "pool_out_weight": heavy_noise(streams_of[12], (P_SIZE, D), P_SIZE ** -0.5, 0.5, ((0, 8), (1, 32)), (0, 1, 32, 2.75), jnp.float32),
        "pool_out_scale": jnp.clip(jnp.exp(math.log(2.0) - 1.3862944 * jax.random.uniform(streams_of[13], (D,), jnp.float32) ** level_of(streams_of[13], (D,), ((0, 8),), -0.2, 0.2)), 0.5, 2.0),
    }


eps = 1e-06
WINDOWS = (2, 4, 8, 16)

def rms_norm(values, norm_gain):
    floats = values.astype(jnp.float32)
    scaled = floats * lax.rsqrt(lax.optimization_barrier(jnp.mean(floats * floats, axis=-1, keepdims=True)) + eps)
    return (scaled * norm_gain).astype(jnp.bfloat16)

def block_sum(left_rows, right_rows, column_scale):
    block_rows = right_rows.shape[0] // N_TP
    running = jnp.zeros((left_rows.shape[0], right_rows.shape[1]), jnp.float32)
    for blocks in range(N_TP):
        block_part = jnp.dot(left_rows[:, blocks * block_rows:(blocks + 1) * block_rows], right_rows[blocks * block_rows:(blocks + 1) * block_rows], preferred_element_type=jnp.float32).astype(jnp.bfloat16)
        block_part = lax.optimization_barrier(block_part)
        running = running + block_part.astype(jnp.float32)
    return running * column_scale

def feed_forward(normed, gate_half, gate_scale, up_half, up_scale, down_half, down_scale):
    gate_sum = jnp.dot(normed, gate_half, preferred_element_type=jnp.float32) * gate_scale
    up_sum = jnp.dot(normed, up_half, preferred_element_type=jnp.float32) * up_scale
    hidden = (jax.nn.silu(gate_sum) * up_sum).astype(jnp.bfloat16)
    return block_sum(hidden, down_half, down_scale)

def pooling(pool_input):
    channels = pool_input.shape[1]
    floats = pool_input.astype(jnp.float32).reshape(-1, SEQ, channels)
    csum = jnp.concatenate([jnp.zeros((floats.shape[0], 1, channels), jnp.float32), jnp.cumsum(floats, axis=1)], axis=1)
    position = jnp.arange(SEQ)
    channel_group = jnp.arange(channels) * 4 // channels
    pooled = -floats
    for group_index, window in enumerate(WINDOWS):
        before = window // 2
        after_span = window - before
        upper_sum = jnp.pad(csum, ((0, 0), (0, after_span), (0, 0)), mode='edge')[:, after_span:after_span + SEQ]
        lower_sum = jnp.pad(csum, ((0, 0), (before, 0), (0, 0)), mode='edge')[:, :SEQ]
        counts = (jnp.minimum(position + after_span, SEQ) - jnp.maximum(position - before, 0)).astype(jnp.float32)
        window_mean = (upper_sum - lower_sum) / counts[None, :, None]
        select = (channel_group == group_index).astype(jnp.float32)
        pooled = pooled + window_mean * select
    return pooled.reshape(-1, channels).astype(jnp.bfloat16)

def reference(stream, gain_first, gain_mixer, gain_second, gate_weight, gate_scale, up_weight, up_scale, down_weight, down_scale, pool_in_weight, pool_in_scale, pool_out_weight, pool_out_scale):
    gate_half = gate_weight.astype(jnp.bfloat16)
    up_half = up_weight.astype(jnp.bfloat16)
    down_half = down_weight.astype(jnp.bfloat16)
    in_half = pool_in_weight.astype(jnp.bfloat16)
    out_half = pool_out_weight.astype(jnp.bfloat16)
    first_branch = feed_forward(rms_norm(stream, gain_first), gate_half, gate_scale, up_half, up_scale, down_half, down_scale)
    after_first = (stream.astype(jnp.float32) + 0.5 * first_branch).astype(jnp.bfloat16)
    mixer_normed = rms_norm(after_first, gain_mixer)
    pool_input = (jnp.dot(mixer_normed, in_half, preferred_element_type=jnp.float32) * pool_in_scale).astype(jnp.bfloat16)
    pooled = pooling(pool_input)
    after_mix = (after_first.astype(jnp.float32) + block_sum(pooled, out_half, pool_out_scale)).astype(jnp.bfloat16)
    second_branch = feed_forward(rms_norm(after_mix, gain_second), gate_half, gate_scale, up_half, up_scale, down_half, down_scale)
    return (after_mix.astype(jnp.float32) + 0.5 * second_branch).astype(jnp.bfloat16)
```

```python
import random

import jax
import jax.numpy as jnp
from jax import lax
from jax.experimental import pallas as pl
from jax.experimental.pallas import tpu as pltpu
from jax.sharding import PartitionSpec as P

SEQ = 128
EPS = 1e-06
WINDOWS = (2, 4, 8, 16)
NZ, NY, NX = 8, 4, 4
ROWS = 384
HALF = ROWS // 2
D = 2048
BLK = 256
FB = 704
GUW = 2 * FB
DH = FB // 2
BF = jnp.bfloat16
F32 = jnp.float32

SIZES = (0.36, 1, 1, 1, 1, 1, 1)
CLASSES = (0, 1, 1, 1, 1, 2, 2)
PIECES_G = (1, 2, 3, 4)
PIECES_D = (5, 6)


def moved(o, d):
    z, y = o
    if d == 0:
        return z, (y + 1) % NY
    if d == 1:
        return z, (y - 1) % NY
    return (z + (1 if d == 2 else -1)) % NZ, y


def broadcast_plan(lag=2.0, seed=43, noise=0.3):
    rng = random.Random(seed)
    count = len(SIZES)
    has = [{(0, 0): 0.0} for _ in range(count)]
    free = [0.0] * 4
    plan = []
    while len(plan) < count * (NZ * NY - 1):
        best = None
        for d in range(4):
            found = []
            for s in range(count):
                for o, t in has[s].items():
                    q = moved(o, d)
                    if q not in has[s]:
                        found.append((max(free[d], t), s, o, q))
            if found:
                first = min(c[0] for c in found)
                if best is None or first < best[0]:
                    best = (first, d, [c for c in found if c[0] <= first + 1e-9])
        _, d, found = best

        def key(c):
            onward = sum(moved(c[3], e) not in has[c[1]] for e in range(4))
            return CLASSES[c[1]], -noise * rng.random() * 4 - onward * 0.5 + len(has[c[1]]) * 0.02

        start, s, o, q = min(found, key=key)
        has[s][q] = start + SIZES[s] + lag
        free[d] = start + SIZES[s]
        plan.append((start, d, s, o))
    return plan, has


def kernel(
    stream, gain1, gainm, gain2, gw, gsc, uw, usc, dw, dsc, iw, isc, ow, osc,
    out,
    gbuf, dbuf, dfull, pall, sall, infull, outfull, xall1, xall2, nbuf, ambuf, hid, ssacc, rst, pacc, pooled,
    snd1, pre1, sr1, rr1, snd2, pre2, sr2, rr2, mine,
    psend, precv, a1s, a1r, a2s, a2r, pas, par, sas, sar, r1s, r1r, r2s, r2r,
):
    f, t = lax.axis_index("fs"), lax.axis_index("tp")
    z, y = f // NY, f % NY
    x, c = t // 2, t % 2
    oc = 1 - c

    def at_f(dz, dy):
        return ((z + dz + NZ) % NZ) * NY + (y + dy + NY) % NY

    def at_t(dx, core):
        return ((x + dx + NX) % NX) * 2 + core

    neighbour = [at_f(0, 1), at_f(0, -1), at_f(1, 0), at_f(-1, 0)]
    right, left, twin = at_t(1, c), at_t(-1, c), at_t(0, oc)

    barrier = pltpu.get_barrier_semaphore()
    for nf in neighbour:
        pl.semaphore_signal(barrier, inc=1, device_id={"fs": nf, "tp": t})
    for nt in (right, left, twin):
        pl.semaphore_signal(barrier, inc=1, device_id={"fs": f, "tp": nt})

    prow = pl.ds(pl.multiple_of(f * 64, 64), 64)
    pall[t, prow, :] = jnp.concatenate([iw[...], ow[...]], axis=1).astype(BF)
    for j in range(5):
        gbuf[prow, 256 * j : 256 * j + 128] = gw[:, 128 * j : 128 * j + 128].astype(BF)
        gbuf[prow, 256 * j + 128 : 256 * j + 256] = uw[:, 128 * j : 128 * j + 128].astype(BF)
    gbuf[prow, 1280:1408] = jnp.concatenate([gw[:, 640:704], uw[:, 640:704]], axis=1).astype(BF)
    dbuf[pl.ds(pl.multiple_of(f * DH, 32), DH), :] = jnp.concatenate([dw[0:DH, :], dw[DH:FB, :]], axis=1).astype(BF)
    xall1[t] = stream[...]
    sall[t] = jnp.concatenate(
        [jnp.broadcast_to(osc[...], (16, 256)), jnp.broadcast_to(isc[...], (16, 64)), jnp.zeros((16, 64), F32)], axis=1
    )
    pl.semaphore_wait(barrier, 7)

    def piece(s, owner):
        if s == 0:
            return pall.at[t, pl.ds(pl.multiple_of(owner * 64, 64), 64), :]
        if s in PIECES_G:
            return gbuf.at[pl.ds(pl.multiple_of(owner * 64 + 16 * (s - 1), 16), 16), :]
        return dbuf.at[pl.ds(pl.multiple_of(owner * DH + 176 * (s - 5), 16), 176), :]

    def owner_of(o):
        return at_f(-o[0], -o[1])

    arrived = set()

    def ensure(s, o):
        if o == (0, 0) or (s, o) in arrived:
            return
        arrived.add((s, o))
        ref = piece(s, owner_of(o))
        pltpu.make_async_remote_copy(
            src_ref=ref, dst_ref=ref, send_sem=psend.at[0], recv_sem=precv.at[s, o[0] * NY + o[1]],
            device_id={"fs": neighbour[0], "tp": t},
        ).wait_recv()

    def send_piece(d, s, o):
        ensure(s, o)
        q = moved(o, d)
        ref = piece(s, owner_of(o))
        pltpu.make_async_remote_copy(
            src_ref=ref, dst_ref=ref, send_sem=psend.at[0 if s == 0 else 1 if s in PIECES_G else 2],
            recv_sem=precv.at[s, q[0] * NY + q[1]], device_id={"fs": neighbour[d], "tp": t},
        ).start()

    class Ring:
        def __init__(self, part, whole, ssem, rsem):
            self.part, self.whole, self.ssem, self.rsem = part, whole, ssem, rsem

        def copy(self, ref, to, rs):
            return pltpu.make_async_remote_copy(
                src_ref=ref, dst_ref=ref, send_sem=self.ssem.at[1 if rs >= 6 else 0], recv_sem=self.rsem.at[rs],
                device_id={"fs": f, "tp": to},
            )

        def start(self):
            me = t
            self.copy(self.part(me, 0), right, 0).start()
            self.copy(self.part(me, 1), left, 3).start()
            self.copy(self.part(me, 1), right, 1).start()
            self.copy(self.part(me, 0), left, 2).start()
            self.copy(self.part(me, 0), twin, 6).start()
            self.copy(self.part(me, 1), twin, 7).start()

        def block(self, k, core):
            return at_t((-1, -1, 1, 1, 2, 2, 0, 0)[k], core), k % 2

        def got(self, k, share=True):
            ref = self.part(*self.block(k, c))
            self.copy(ref, twin, k).wait_recv()
            if k == 0:
                self.copy(ref, right, 4).start()
            if k == 3:
                self.copy(ref, left, 5).start()
            if share:
                self.copy(ref, twin, 8 + k).start()

        def got_twin(self, k):
            ref = self.part(*self.block(k, oc))
            self.copy(ref, twin, 8 + k if k < 6 else k).wait_recv()

        def done(self):
            pltpu.make_async_remote_copy(
                src_ref=self.whole(3), dst_ref=self.whole(3), send_sem=self.ssem.at[0], recv_sem=self.rsem.at[0],
                device_id={"fs": f, "tp": twin},
            ).wait_send()
            pltpu.make_async_remote_copy(
                src_ref=self.whole(4), dst_ref=self.whole(4), send_sem=self.ssem.at[1], recv_sem=self.rsem.at[0],
                device_id={"fs": f, "tp": twin},
            ).wait_send()

    def halves(buf, size):
        return (
            lambda b, h: buf.at[b, pl.ds(h * (size // 2), size // 2), :],
            lambda n: buf.at[pl.ds(0, n)],
        )

    ag1 = Ring(*halves(xall1, ROWS), a1s, a1r)
    ag2 = Ring(*halves(xall2, ROWS), a2s, a2r)
    pag = Ring(*halves(pall, D), pas, par)
    sag = Ring(*halves(sall, 16), sas, sar)
    sag.part = lambda b, h: sall.at[b, pl.ds(h * 8, 8), :]

    def norm_block(b, src, gain, first):
        v = src[b].astype(F32)
        sq = v * v
        sq = sq[:, :128] + sq[:, 128:]
        ssacc[...] = sq if first else ssacc[...] + sq
        return (v * gain[:, b * BLK : (b + 1) * BLK]).astype(BF)

    def finish_norm():
        mean = jnp.sum(ssacc[...], axis=1, keepdims=True) * (1.0 / D)
        rst[...] = jnp.broadcast_to(lax.rsqrt(mean + EPS), (ROWS, 128))

    def norm1(b):
        nbuf[:, b * BLK : (b + 1) * BLK] = norm_block(b, xall1, gain1, b == 0)

    def hidden(j):
        if j < 5:
            acc = jnp.dot(nbuf[...], gbuf[:, 256 * j : 256 * j + 256], preferred_element_type=F32)
            r = rst[...]
            g = acc[:, :128] * r * gsc[:, 128 * j : 128 * j + 128]
            u = acc[:, 128:] * r * usc[:, 128 * j : 128 * j + 128]
            hid[:, 128 * j : 128 * j + 128] = (g / (1.0 + jnp.exp(-g)) * u).astype(BF)
        else:
            acc = jnp.dot(nbuf[...], gbuf[:, 1280:1408], preferred_element_type=F32)
            scale = jnp.concatenate([gsc[:, 640:704], usc[:, 640:704]], axis=1)
            v = acc * rst[...] * scale
            u = pltpu.roll(v, 64, 1)
            h = v / (1.0 + jnp.exp(-v)) * u
            lane = lax.broadcasted_iota(jnp.int32, h.shape, 1)
            hid[:, 640:768] = jnp.where(lane < 64, h, 0.0).astype(BF)

    def unpack_down(b):
        for pair in range(2):
            one = dbuf[pl.ds(pl.multiple_of((4 * b + 2 * pair) * DH, 32), DH), :]
            two = dbuf[pl.ds(pl.multiple_of((4 * b + 2 * pair + 1) * DH, 32), DH), :]
            cols = slice(128 * pair, 128 * pair + 128)
            dfull[b, 0:DH, cols] = jnp.concatenate([one[:, :64], two[:, :64]], axis=1)
            dfull[b, DH:FB, cols] = jnp.concatenate([one[:, 64:], two[:, 64:]], axis=1)

    def unpack_in(k):
        rows = pl.ds(256 * k, 256)
        for i in range(NX):
            infull[rows, 128 * i : 128 * i + 128] = jnp.concatenate(
                [pall[2 * i, rows, :][:, :64], pall[2 * i + 1, rows, :][:, :64]], axis=1
            )

    def unpack_out(b):
        for i in range(16):
            outfull[64 * b : 64 * b + 64, 128 * i : 128 * i + 128] = jnp.concatenate(
                [pall[b, 128 * i : 128 * i + 64, :][:, 64:], pall[b, 128 * i + 64 : 128 * i + 128, :][:, 64:]], axis=1
            )

    def down(b):
        return jnp.dot(hid[...], dfull[b], preferred_element_type=F32)

    def summed_down(snd, pre, sr, rr, ss, rs):
        offs = (0, 1, 2, -1)
        A, B = pl.ds(0, HALF), pl.ds(HALF, HALF)

        def to_twin(k):
            snd[k] = down(at_t(offs[k], oc)).astype(BF)
            pltpu.make_async_remote_copy(
                src_ref=snd.at[k], dst_ref=pre.at[k], send_sem=ss.at[0], recv_sem=rs.at[k],
                device_id={"fs": f, "tp": twin},
            ).start()

        def own(k):
            mine[k] = down(at_t(offs[k], c))

        def both(k):
            pltpu.make_async_remote_copy(
                src_ref=snd.at[k], dst_ref=pre.at[k], send_sem=ss.at[0], recv_sem=rs.at[k],
                device_id={"fs": f, "tp": twin},
            ).wait_recv()

        def hop(src, slot, rows, sem, to):
            return pltpu.make_async_remote_copy(
                src_ref=src, dst_ref=rr.at[slot, rows, :], send_sem=ss.at[1], recv_sem=rs.at[sem],
                device_id={"fs": f, "tp": to},
            )

        to_twin(2)
        to_twin(1)
        own(2)
        both(2)
        sr[2] = (mine[2] + pre[2].astype(F32)).astype(BF)
        hop(sr.at[2, A, :], 2, A, 4, right).start()
        hop(sr.at[2, B, :], 2, B, 5, left).start()
        to_twin(3)
        own(1)
        both(1)
        sr[1, B, :] = (mine[1, B, :] + pre[1, B, :].astype(F32)).astype(BF)
        hop(sr.at[1, B, :], 0, B, 6, right).start()
        own(3)
        both(3)
        sr[0, A, :] = (mine[3, A, :] + pre[3, A, :].astype(F32)).astype(BF)
        hop(sr.at[0, A, :], 1, A, 7, left).start()
        to_twin(0)
        own(0)
        hop(sr.at[2, A, :], 2, A, 4, right).wait_recv()
        sr[1, A, :] = (mine[1, A, :] + pre[1, A, :].astype(F32) + rr[2, A, :].astype(F32)).astype(BF)
        hop(sr.at[1, A, :], 0, A, 8, right).start()
        hop(sr.at[2, B, :], 2, B, 5, left).wait_recv()
        sr[0, B, :] = (mine[3, B, :] + pre[3, B, :].astype(F32) + rr[2, B, :].astype(F32)).astype(BF)
        hop(sr.at[0, B, :], 1, B, 9, left).start()
        both(0)
        mine[0] = mine[0] + pre[0].astype(F32)
        hop(sr.at[1, B, :], 0, B, 6, right).wait_recv()
        hop(sr.at[0, A, :], 1, A, 7, left).wait_recv()
        hop(sr.at[1, A, :], 0, A, 8, right).wait_recv()
        hop(sr.at[0, B, :], 1, B, 9, left).wait_recv()
        mine[0] = mine[0] + rr[0].astype(F32) + rr[1].astype(F32)

    def summed_done(snd, sr, ss, rs):
        for ref, k in ((snd.at[pl.ds(0, 4)], 0), (sr.at[pl.ds(0, 3)], 1)):
            pltpu.make_async_remote_copy(
                src_ref=ref, dst_ref=ref, send_sem=ss.at[k], recv_sem=rs.at[0], device_id={"fs": f, "tp": twin}
            ).wait_send()

    plan, has = broadcast_plan()
    events = []

    def when(time, fn):
        events.append((time, len(events), fn))

    for start, d, s, o in plan:
        when(start, lambda d=d, s=s, o=o: send_piece(d, s, o))

    when(1.5, ag1.start)
    when(1.6, sag.start)
    for k, time in ((0, 5.5), (3, 5.5), (1, 8.5), (2, 8.5), (4, 11.0), (5, 11.0)):
        when(time, lambda k=k: ag1.got(k))
        when(time + 0.01, lambda k=k: sag.got(k))

    def twin1():
        for k in range(8):
            ag1.got_twin(k)
            sag.got_twin(k)

    when(13.0, twin1)
    for b in range(8):
        when(13.2 + 0.6 * b, lambda b=b: norm1(b))
    when(18.2, finish_norm)

    p_done = max(has[0].values())

    def pool_ring():
        for o in has[0]:
            ensure(0, o)
        pag.start()

    when(p_done, pool_ring)
    for k, time in ((0, 8.5), (3, 8.5), (1, 14.5), (2, 14.5), (4, 20.5), (5, 20.5)):
        when(p_done + time, lambda k=k: pag.got(k))

    def twin_pool():
        for k in range(8):
            pag.got_twin(k)

    when(p_done + 24.0, twin_pool)
    for b in range(8):
        when(p_done + 24.5 + b, lambda b=b: unpack_in(b))
        when(p_done + 25.0 + b, lambda b=b: unpack_out(b))

    g_done = max(max(has[s].values()) for s in PIECES_G)

    def gates():
        for s in PIECES_G:
            for o in has[s]:
                ensure(s, o)

    when(g_done, gates)
    for j in range(6):
        when(g_done + 0.1 + 1.5 * j, lambda j=j: hidden(j))

    def plane(oz):
        for s in PIECES_D:
            for oy in range(NY):
                ensure(s, (oz, oy))
        unpack_down((z - oz + NZ) % NZ)

    def clear_down():
        dfull[:, FB:768, :] = jnp.zeros((8, 768 - FB, BLK), BF)

    when(0.5, clear_down)
    for oz in range(NZ):
        when(max(has[s][oz, oy] for s in PIECES_D for oy in range(NY)), lambda oz=oz: plane(oz))

    for _, _, fn in sorted(events, key=lambda e: e[:2]):
        fn()

    summed_down(snd1, pre1, sr1, rr1, r1s, r1r)
    xall2[t] = (stream[...].astype(F32) + 0.5 * (mine[0] * dsc[...])).astype(BF)
    ag2.start()
    for k in (0, 3, 1, 2, 4, 5):
        ag2.got(k)
    for k in (6, 7, 0, 3, 1, 2, 4, 5):
        ag2.got_twin(k)

    for b in range(8):
        v = norm_block(b, xall2, gainm, b == 0)
        part = jnp.dot(v, infull[b * BLK : (b + 1) * BLK, :], preferred_element_type=F32)
        pacc[...] = part if b == 0 else pacc[...] + part
    finish_norm()
    row = lax.broadcasted_iota(jnp.int32, (SEQ, SEQ), 0)
    col = lax.broadcasted_iota(jnp.int32, (SEQ, SEQ), 1)
    for g, window in enumerate(WINDOWS):
        low = jnp.maximum(row - window // 2, 0)
        high = jnp.minimum(row + window - window // 2, SEQ)
        band = jnp.where((col >= low) & (col < high), 1.0, 0.0).astype(BF)
        count = (high - low).astype(F32)
        scale = jnp.concatenate([sall[2 * g, 0:1, 256:320], sall[2 * g + 1, 0:1, 256:320]], axis=1)
        cols = slice(128 * g, 128 * g + 128)
        for q in range(ROWS // SEQ):
            rows = slice(SEQ * q, SEQ * q + SEQ)
            value = (pacc[rows, cols] * rst[rows, :] * scale).astype(BF)
            total = jnp.dot(band, value, preferred_element_type=F32)
            pooled[rows, cols] = (total / count - value.astype(F32)).astype(BF)
    for b in range(8):
        cols = slice(b * BLK, (b + 1) * BLK)
        mix = jnp.dot(pooled[...], outfull[:, cols], preferred_element_type=F32)
        v = (xall2[b].astype(F32) + mix * sall[b, 0:1, 0:256]).astype(BF)
        ambuf[b] = v
        nbuf[:, cols] = norm_block(b, ambuf, gain2, b == 0)
    finish_norm()

    for j in range(6):
        hidden(j)
    summed_down(snd2, pre2, sr2, rr2, r2s, r2r)
    out[...] = (ambuf[t].astype(F32) + 0.5 * (mine[0] * dsc[...])).astype(BF)

    for ref, k in ((pall.at[0, pl.ds(0, 31 * 64), :], 0), (gbuf.at[pl.ds(0, 124 * 16), :], 1), (dbuf.at[pl.ds(0, 62 * 176), :], 2)):
        pltpu.make_async_remote_copy(
            src_ref=ref, dst_ref=ref, send_sem=psend.at[k], recv_sem=precv.at[0, 0], device_id={"fs": neighbour[0], "tp": t}
        ).wait_send()
    for ring in (ag1, sag, pag, ag2):
        ring.done()
    summed_done(snd1, sr1, r1s, r1r)
    summed_done(snd2, sr2, r2s, r2r)


def body(
    stream, gain_first, gain_mixer, gain_second, gate_weight, gate_scale, up_weight, up_scale,
    down_weight, down_scale, pool_in_weight, pool_in_scale, pool_out_weight, pool_out_scale,
):
    def line(v):
        return v.reshape(1, -1)

    vmem = pl.BlockSpec(memory_space=pltpu.VMEM)
    V = pltpu.VMEM
    sem = pltpu.SemaphoreType.DMA
    exchange = [V((4, ROWS, BLK), BF), V((4, ROWS, BLK), BF), V((3, ROWS, BLK), BF), V((3, ROWS, BLK), BF)]
    ring_sems = [sem((2,)), sem((14,))]
    return pl.pallas_call(
        kernel,
        out_shape=jax.ShapeDtypeStruct((ROWS, BLK), BF),
        in_specs=[vmem] * 14,
        out_specs=vmem,
        scratch_shapes=[
            V((D, GUW), BF),
            V((32 * DH, 128), BF),
            V((8, 768, BLK), BF),
            V((8, D, 128), BF),
            V((8, 16, 384), F32),
            V((D, 512), BF),
            V((512, D), BF),
            V((8, ROWS, BLK), BF),
            V((8, ROWS, BLK), BF),
            V((ROWS, D), BF),
            V((8, ROWS, BLK), BF),
            V((ROWS, 768), BF),
            V((ROWS, 128), F32),
            V((ROWS, 128), F32),
            V((ROWS, 512), F32),
            V((ROWS, 512), BF),
            *exchange,
            *exchange,
            V((4, ROWS, BLK), F32),
            sem((3,)), sem((7, 32)),
            *ring_sems, *ring_sems, *ring_sems, *ring_sems,
            sem((2,)), sem((10,)), sem((2,)), sem((10,)),
        ],
        compiler_params=pltpu.CompilerParams(
            collective_id=0, has_side_effects=True, vmem_limit_bytes=60 * 1024 * 1024
        ),
    )(
        stream, line(gain_first), line(gain_mixer), line(gain_second), gate_weight, line(gate_scale), up_weight,
        line(up_scale), down_weight, line(down_scale), pool_in_weight, line(pool_in_scale), pool_out_weight,
        line(pool_out_scale),
    )


def solution(mesh):
    placed = (
        P("fs", "tp"), P(), P(), P(), P("fs", "tp"), P("tp"), P("fs", "tp"), P("tp"), P("tp", "fs"), P("tp"),
        P("fs", "tp"), P("tp"), P("tp", "fs"), P("tp"),
    )
    return jax.shard_map(body, mesh=mesh, in_specs=placed, out_specs=P("fs", "tp"), check_vma=False)
```

```python
import random

import jax
import jax.numpy as jnp
from jax import lax
from jax.experimental import pallas as pl
from jax.experimental.pallas import tpu as pltpu
from jax.sharding import PartitionSpec as P

SEQ = 128
EPS = 1e-06
WINDOWS = (2, 4, 8, 16)
NZ, NY, NX = 8, 4, 4
ROWS = 384
HALF = ROWS // 2
D = 2048
BLK = 256
FB = 704
GUW = 2 * FB
DH = FB // 2
BF = jnp.bfloat16
F32 = jnp.float32

SIZES = (0.36, 1, 1, 1, 1, 1, 1)
RANKS = (-1, 0, 0, 0, 0, 1, 1)
PIECES_G = (1, 2, 3, 4)
PIECES_D = (5, 6)
PLAN = (4.0, 345, 1.0)
G_LATE, D_LATE = 1.0, 0.5


def moved(o, d):
    z, y = o
    if d == 0:
        return z, (y + 1) % NY
    if d == 1:
        return z, (y - 1) % NY
    return (z + (1 if d == 2 else -1)) % NZ, y


def broadcast_plan(lag=PLAN[0], seed=PLAN[1], noise=PLAN[2]):
    rng = random.Random(seed)
    count = len(SIZES)
    has = [{(0, 0): 0.0} for _ in range(count)]
    free = [0.0] * 4
    plan = []
    while len(plan) < count * (NZ * NY - 1):
        best = None
        for d in range(4):
            found = []
            for s in range(count):
                for o, t in has[s].items():
                    q = moved(o, d)
                    if q not in has[s]:
                        found.append((max(free[d], t), s, o, q))
            if found:
                first = min(c[0] for c in found)
                if best is None or first < best[0]:
                    best = (first, d, [c for c in found if c[0] <= first + 1e-9])
        _, d, found = best

        def key(c):
            onward = sum(moved(c[3], e) not in has[c[1]] for e in range(4))
            return RANKS[c[1]] * 1.5 - noise * rng.random() * 4 - onward * 0.5 + len(has[c[1]]) * 0.02

        start, s, o, q = min(found, key=key)
        has[s][q] = start + SIZES[s] + lag
        free[d] = start + SIZES[s]
        plan.append((start, d, s, o))
    return plan, has


def kernel(
    stream, gain1, gainm, gain2, gw, gsc1, uw, usc1, dw, dsc, iw, isc, ow, osc,
    out,
    gbuf, dbuf, dfull, pall, sall, infull, outfull, xall1, xall2, nbuf, ambuf, hid, ssacc, rst, pacc, pooled,
    snd1, pre1, sr1, rr1, snd2, pre2, sr2, rr2, mine, tot,
    gsc, usc, psend, precv, a1s, a1r, a2s, a2r, pas, par, sas, sar, r1s, r1r, r2s, r2r,
):
    f, t = lax.axis_index("fs"), lax.axis_index("tp")
    z, y = f // NY, f % NY
    x, c = t // 2, t % 2
    oc = 1 - c

    def at_f(dz, dy):
        return ((z + dz + NZ) % NZ) * NY + (y + dy + NY) % NY

    def at_t(dx, core):
        return ((x + dx + NX) % NX) * 2 + core

    neighbour = [at_f(0, 1), at_f(0, -1), at_f(1, 0), at_f(-1, 0)]
    right, left, twin = at_t(1, c), at_t(-1, c), at_t(0, oc)

    barrier = pltpu.get_barrier_semaphore()
    for nf in neighbour:
        pl.semaphore_signal(barrier, inc=1, device_id={"fs": nf, "tp": t})
    for nt in (right, left, twin):
        pl.semaphore_signal(barrier, inc=1, device_id={"fs": f, "tp": nt})

    prow = pl.ds(pl.multiple_of(f * 64, 64), 64)
    pall[t, prow, :] = jnp.concatenate([iw[...], ow[...]], axis=1).astype(BF)
    for j in range(5):
        gbuf[prow, 256 * j : 256 * j + 128] = gw[:, 128 * j : 128 * j + 128].astype(BF)
        gbuf[prow, 256 * j + 128 : 256 * j + 256] = uw[:, 128 * j : 128 * j + 128].astype(BF)
    gbuf[prow, 1280:1408] = jnp.concatenate([gw[:, 640:704], uw[:, 640:704]], axis=1).astype(BF)
    down_rows = jnp.transpose(dw[...])
    dbuf[pl.ds(pl.multiple_of(f * DH, 32), DH), :] = jnp.concatenate([down_rows[0:DH, :], down_rows[DH:FB, :]], axis=1).astype(BF)
    xall1[t] = stream[...]
    sall[t] = jnp.concatenate(
        [jnp.broadcast_to(osc[...], (16, 256)), jnp.broadcast_to(isc[...], (16, 64)), jnp.zeros((16, 64), F32)], axis=1
    )
    gsc[...] = gsc1[...].reshape(1, FB)
    usc[...] = usc1[...].reshape(1, FB)
    pl.semaphore_wait(barrier, 7)

    def piece(s, owner):
        if s == 0:
            return pall.at[t, pl.ds(pl.multiple_of(owner * 64, 64), 64), :]
        if s in PIECES_G:
            return gbuf.at[pl.ds(pl.multiple_of(owner * 64 + 16 * (s - 1), 16), 16), :]
        return dbuf.at[pl.ds(pl.multiple_of(owner * DH + 176 * (s - 5), 16), 176), :]

    def owner_of(o):
        return at_f(-o[0], -o[1])

    arrived = set()

    def ensure(s, o):
        if o == (0, 0) or (s, o) in arrived:
            return
        arrived.add((s, o))
        ref = piece(s, owner_of(o))
        pltpu.make_async_remote_copy(
            src_ref=ref, dst_ref=ref, send_sem=psend.at[0], recv_sem=precv.at[s, o[0] * NY + o[1]],
            device_id={"fs": neighbour[0], "tp": t},
        ).wait_recv()

    def send_piece(d, s, o):
        ensure(s, o)
        q = moved(o, d)
        ref = piece(s, owner_of(o))
        pltpu.make_async_remote_copy(
            src_ref=ref, dst_ref=ref, send_sem=psend.at[0 if s == 0 else 1 if s in PIECES_G else 2],
            recv_sem=precv.at[s, q[0] * NY + q[1]], device_id={"fs": neighbour[d], "tp": t},
        ).start()

    class Ring:
        def __init__(self, part, whole, ssem, rsem, base=0):
            self.part, self.whole, self.ssem, self.rsem, self.base = part, whole, ssem, rsem, base

        def copy(self, ref, to, rs):
            return pltpu.make_async_remote_copy(
                src_ref=ref, dst_ref=ref, send_sem=self.ssem.at[1 if rs >= 6 else 0], recv_sem=self.rsem.at[self.base + rs],
                device_id={"fs": f, "tp": to},
            )

        def start(self):
            me = t
            self.copy(self.part(me, 0), right, 0).start()
            self.copy(self.part(me, 1), left, 3).start()
            self.copy(self.part(me, 1), right, 1).start()
            self.copy(self.part(me, 0), left, 2).start()
            self.copy(self.part(me, 0), twin, 6).start()
            self.copy(self.part(me, 1), twin, 7).start()

        def block(self, k, core):
            return at_t((-1, -1, 1, 1, 2, 2, 0, 0)[k], core), k % 2

        def got(self, k, share=True):
            ref = self.part(*self.block(k, c))
            self.copy(ref, twin, k).wait_recv()
            if k == 0:
                self.copy(ref, right, 4).start()
            if k == 3:
                self.copy(ref, left, 5).start()
            if share:
                self.copy(ref, twin, 8 + k).start()

        def got_twin(self, k):
            ref = self.part(*self.block(k, oc))
            self.copy(ref, twin, 8 + k if k < 6 else k).wait_recv()

        def done(self):
            pltpu.make_async_remote_copy(
                src_ref=self.whole(3), dst_ref=self.whole(3), send_sem=self.ssem.at[0], recv_sem=self.rsem.at[0],
                device_id={"fs": f, "tp": twin},
            ).wait_send()
            pltpu.make_async_remote_copy(
                src_ref=self.whole(4), dst_ref=self.whole(4), send_sem=self.ssem.at[1], recv_sem=self.rsem.at[0],
                device_id={"fs": f, "tp": twin},
            ).wait_send()

    def halves(buf, size):
        return (
            lambda b, h: buf.at[b, pl.ds(h * (size // 2), size // 2), :],
            lambda n: buf.at[pl.ds(0, n)],
        )

    ag1 = Ring(*halves(xall1, ROWS), a1s, a1r)
    pag = Ring(*halves(pall, D), pas, par)
    sag = Ring(*halves(sall, 16), sas, sar)
    sag.part = lambda b, h: sall.at[b, pl.ds(h * 8, 8), :]

    def norm_block(b, src, gain, first):
        v = src[b].astype(F32)
        sq = v * v
        sq = sq[:, :128] + sq[:, 128:]
        ssacc[...] = sq if first else ssacc[...] + sq
        return (v * gain[:, b * BLK : (b + 1) * BLK]).astype(BF)

    def finish_norm():
        mean = jnp.sum(ssacc[...], axis=1, keepdims=True) * (1.0 / D)
        rst[...] = jnp.broadcast_to(lax.rsqrt(mean + EPS), (ROWS, 128))

    def norm1(b):
        nbuf[:, b * BLK : (b + 1) * BLK] = norm_block(b, xall1, gain1, b == 0)

    def hidden(j, at=0, size=ROWS):
        rows = slice(at, at + size)
        r = rst[rows, :]
        if j < 5:
            acc = jnp.dot(nbuf[rows, :], gbuf[:, 256 * j : 256 * j + 256], preferred_element_type=F32)
            g = acc[:, :128] * r * gsc[:, 128 * j : 128 * j + 128]
            u = acc[:, 128:] * r * usc[:, 128 * j : 128 * j + 128]
            hid[rows, 128 * j : 128 * j + 128] = (g / (1.0 + jnp.exp(-g)) * u).astype(BF)
        else:
            acc = jnp.dot(nbuf[rows, :], gbuf[:, 1280:1408], preferred_element_type=F32)
            scale = jnp.concatenate([gsc[:, 640:704], usc[:, 640:704]], axis=1)
            v = acc * r * scale
            u = pltpu.roll(v, 64, 1)
            h = v / (1.0 + jnp.exp(-v)) * u
            lane = lax.broadcasted_iota(jnp.int32, h.shape, 1)
            hid[rows, 640:768] = jnp.where(lane < 64, h, 0.0).astype(BF)

    def unpack_down(b):
        side = (b + c) % 2
        for pair in range(2):
            one = dbuf[pl.ds(pl.multiple_of((4 * b + 2 * pair) * DH, 32), DH), :]
            two = dbuf[pl.ds(pl.multiple_of((4 * b + 2 * pair + 1) * DH, 32), DH), :]
            cols = pl.ds(pl.multiple_of(side * BLK + 128 * pair, 128), 128)
            dfull[b // 2, 0:DH, cols] = jnp.concatenate([one[:, :64], two[:, :64]], axis=1)
            dfull[b // 2, DH:FB, cols] = jnp.concatenate([one[:, 64:], two[:, 64:]], axis=1)

    def unpack_in(k):
        rows = pl.ds(256 * k, 256)
        for i in range(NX):
            infull[rows, 128 * i : 128 * i + 128] = jnp.concatenate(
                [pall[2 * i, rows, :][:, :64], pall[2 * i + 1, rows, :][:, :64]], axis=1
            )

    def unpack_out(b):
        for i in range(16):
            outfull[64 * b : 64 * b + 64, 128 * i : 128 * i + 128] = jnp.concatenate(
                [pall[b, 128 * i : 128 * i + 64, :][:, 64:], pall[b, 128 * i + 64 : 128 * i + 128, :][:, 64:]], axis=1
            )

    def down(chip, cols):
        return jnp.dot(hid[...], dfull[chip, :, cols], preferred_element_type=F32)

    OWN, OTHER = slice(0, BLK), slice(BLK, 2 * BLK)

    SEQS = range(ROWS // SEQ)

    class Sum:
        def __init__(self, snd, pre, sr, rr, ss, rs):
            self.snd, self.pre, self.sr, self.rr, self.ss, self.rs = snd, pre, sr, rr, ss, rs

        def pair(self, k):
            return pltpu.make_async_remote_copy(
                src_ref=self.snd.at[k], dst_ref=self.pre.at[k], send_sem=self.ss.at[0], recv_sem=self.rs.at[k],
                device_id={"fs": f, "tp": twin},
            )

        def half(self, q, h):
            return pl.ds(SEQ * q + h * (SEQ // 2), SEQ // 2)

        def hop(self, q, src, slot, h, sem, to):
            rows = self.half(q, h)
            return pltpu.make_async_remote_copy(
                src_ref=self.sr.at[src, rows, :], dst_ref=self.rr.at[slot, rows, :], send_sem=self.ss.at[1],
                recv_sem=self.rs.at[4 + 6 * q + sem], device_id={"fs": f, "tp": to},
            )

        def far(self, total):
            self.sr[2] = total.astype(BF)
            for q in SEQS:
                self.hop(q, 2, 2, 0, 0, right).start()
                self.hop(q, 2, 2, 1, 1, left).start()

        def near_right(self, total):
            tot[1] = total
            for q in SEQS:
                rows = self.half(q, 1)
                self.sr[1, rows, :] = tot[1, rows, :].astype(BF)
                self.hop(q, 1, 0, 1, 2, right).start()

        def near_left(self, total):
            tot[3] = total
            for q in SEQS:
                rows = self.half(q, 0)
                self.sr[0, rows, :] = tot[3, rows, :].astype(BF)
                self.hop(q, 0, 1, 0, 3, left).start()

        def through(self, q):
            rows = self.half(q, 0)
            self.hop(q, 2, 2, 0, 0, right).wait_recv()
            self.sr[1, rows, :] = (tot[1, rows, :] + self.rr[2, rows, :].astype(F32)).astype(BF)
            self.hop(q, 1, 0, 0, 4, right).start()
            rows = self.half(q, 1)
            self.hop(q, 2, 2, 1, 1, left).wait_recv()
            self.sr[0, rows, :] = (tot[3, rows, :] + self.rr[2, rows, :].astype(F32)).astype(BF)
            self.hop(q, 0, 1, 1, 5, left).start()

        def total(self, q):
            self.hop(q, 1, 0, 1, 2, right).wait_recv()
            self.hop(q, 0, 1, 0, 3, left).wait_recv()
            self.hop(q, 1, 0, 0, 4, right).wait_recv()
            self.hop(q, 0, 1, 1, 5, left).wait_recv()
            rows = pl.ds(SEQ * q, SEQ)
            return tot[0, rows, :] + self.rr[0, rows, :].astype(F32) + self.rr[1, rows, :].astype(F32)

        def done(self):
            for ref, k in ((self.snd.at[pl.ds(0, 4)], 0), (self.sr.at[pl.ds(0, 3)], 1)):
                pltpu.make_async_remote_copy(
                    src_ref=ref, dst_ref=ref, send_sem=self.ss.at[k], recv_sem=self.rs.at[0],
                    device_id={"fs": f, "tp": twin},
                ).wait_send()

    first = Sum(snd1, pre1, sr1, rr1, r1s, r1r)
    second = Sum(snd2, pre2, sr2, rr2, r2s, r2r)

    plan, has = broadcast_plan()
    events = []

    def when(time, fn):
        events.append((time, len(events), fn))

    for start, d, s, o in plan:
        when(start, lambda d=d, s=s, o=o: send_piece(d, s, o))

    when(1.5, ag1.start)
    when(1.6, sag.start)
    for k, time in ((0, 5.5), (3, 5.5), (1, 8.5), (2, 8.5), (4, 11.0), (5, 11.0)):
        when(time, lambda k=k: ag1.got(k))
        when(time + 0.01, lambda k=k: sag.got(k))

    def twin1():
        for k in range(8):
            ag1.got_twin(k)
            sag.got_twin(k)

    when(13.0, twin1)
    for b in range(8):
        when(13.2 + 0.6 * b, lambda b=b: norm1(b))
    when(18.2, finish_norm)

    p_done = max(has[0].values())

    def pool_ring():
        for o in has[0]:
            ensure(0, o)
        pag.start()

    when(p_done, pool_ring)
    for k, time in ((0, 8.5), (3, 8.5), (1, 15.0), (2, 15.0), (4, 22.5), (5, 22.5)):
        when(p_done + time, lambda k=k: pag.got(k))

    def twin_pool():
        for k in range(8):
            pag.got_twin(k)

    when(70.0, twin_pool)
    for b in range(8):
        when(70.1, lambda b=b: unpack_in(b))
        when(70.2, lambda b=b: unpack_out(b))

    g_done = max(max(has[s].values()) for s in PIECES_G)

    def gates():
        for s in PIECES_G:
            for o in has[s]:
                ensure(s, o)

    when(g_done + G_LATE, gates)

    def hidden_part(js):
        for j in js:
            hidden(j)

    when(g_done + G_LATE + 0.1, lambda: hidden_part((0, 1, 2)))
    when(g_done + G_LATE + 1.9, lambda: hidden_part((3, 4, 5)))

    def plane(oz):
        for s in PIECES_D:
            for oy in range(NY):
                ensure(s, (oz, oy))
        unpack_down((z - oz + NZ) % NZ)

    def clear_down():
        dfull[:, FB:768, :] = jnp.zeros((NX, 768 - FB, 2 * BLK), BF)

    when(0.5, clear_down)
    ready = {oz: max(has[s][oz, oy] for s in PIECES_D for oy in range(NY)) for oz in range(NZ)}
    even, odd = (sorted(range(e, NZ, 2), key=lambda oz: ready[oz]) for e in (0, 1))
    turn = (z + c) % 2

    def products(i):
        one, two = (z - even[i] + NZ) % NZ, (z - odd[i] + NZ) % NZ
        for_twin = one * turn + two * (1 - turn)
        own = two * turn + one * (1 - turn)
        snd1[i] = down(for_twin // 2, OTHER).astype(BF)
        first.pair(i).start()
        mine[i] = down(own // 2, OWN)

    def combine(i):
        one, two = (z - even[i] + NZ) % NZ, (z - odd[i] + NZ) % NZ
        own = two * turn + one * (1 - turn)
        away = (own // 2 - x + NX) % NX
        first.pair(i).wait_recv()
        mine[i] = mine[i] + pre1[i].astype(F32)

        @pl.when(away == 2)
        def _():
            first.far(mine[i])

        @pl.when(away == 1)
        def _():
            first.near_right(mine[i])

        @pl.when(away == 3)
        def _():
            first.near_left(mine[i])

        @pl.when(away == 0)
        def _():
            tot[0] = mine[i]

    hid_done = g_done + G_LATE + 3.6
    for oz in range(NZ):
        when(ready[oz] + D_LATE, lambda oz=oz: plane(oz))
    for i in range(4):
        at = max(hid_done + 1.0 * i, max(ready[even[i]], ready[odd[i]]) + D_LATE + 0.01)
        when(at, lambda i=i: products(i))
        when(at + 1.6, lambda i=i: combine(i))

    for _, _, fn in sorted(events, key=lambda e: e[:2]):
        fn()

    for q in SEQS:
        first.through(q)
    gathers = []
    for q in SEQS:
        gather = Ring(
            lambda b, h, q=q: xall2.at[b, pl.ds(SEQ * q + h * (SEQ // 2), SEQ // 2), :],
            lambda n: xall2.at[pl.ds(0, n)], a2s, a2r, 14 * q,
        )
        gathers.append(gather)
        rows = pl.ds(SEQ * q, SEQ)
        xall2[t, rows, :] = (stream[rows, :].astype(F32) + 0.5 * (first.total(q) * dsc[...])).astype(BF)
        gather.start()

    def enter(b, start=False):
        v = xall2[b].astype(F32)
        sq = v * v
        sq = sq[:, :128] + sq[:, 128:]
        at = pl.multiple_of(b * BLK, BLK)
        w = (v * gainm[:, pl.ds(at, BLK)]).astype(BF)
        part = jnp.dot(w, infull[pl.ds(at, BLK), :], preferred_element_type=F32)
        ssacc[...] = sq if start else ssacc[...] + sq
        pacc[...] = part if start else pacc[...] + part

    enter(t, True)
    for q in SEQS:
        for k in (0, 3):
            gathers[q].got(k)
    for q in SEQS:
        gathers[q].got_twin(6)
        gathers[q].got_twin(7)
    enter(twin)
    for q in SEQS:
        for k in (1, 2):
            gathers[q].got(k)
    enter(left)
    enter(right)
    for q in SEQS:
        for k in (0, 1, 2, 3):
            gathers[q].got_twin(k)
    enter(at_t(-1, oc))
    enter(at_t(1, oc))
    for q in SEQS:
        for k in (4, 5):
            gathers[q].got(k)
    enter(at_t(2, c))
    for q in SEQS:
        for k in (4, 5):
            gathers[q].got_twin(k)
    enter(at_t(2, oc))
    finish_norm()
    row = lax.broadcasted_iota(jnp.int32, (SEQ, SEQ), 0)
    col = lax.broadcasted_iota(jnp.int32, (SEQ, SEQ), 1)
    for g, window in enumerate(WINDOWS):
        low = jnp.maximum(row - window // 2, 0)
        high = jnp.minimum(row + window - window // 2, SEQ)
        band = jnp.where((col >= low) & (col < high), 1.0, 0.0).astype(BF)
        count = (high - low).astype(F32)
        scale = jnp.concatenate([sall[2 * g, 0:1, 256:320], sall[2 * g + 1, 0:1, 256:320]], axis=1)
        cols = slice(128 * g, 128 * g + 128)
        for q in SEQS:
            rows = slice(SEQ * q, SEQ * q + SEQ)
            value = (pacc[rows, cols] * rst[rows, :] * scale).astype(BF)
            whole = jnp.dot(band, value, preferred_element_type=F32)
            pooled[rows, cols] = (whole / count - value.astype(F32)).astype(BF)
    for b in range(8):
        cols = slice(b * BLK, (b + 1) * BLK)
        mix = jnp.dot(pooled[...], outfull[:, cols], preferred_element_type=F32)
        v = (xall2[b].astype(F32) + mix * sall[b, 0:1, 0:256]).astype(BF)
        ambuf[b] = v
        nbuf[:, cols] = norm_block(b, ambuf, gain2, b == 0)
    finish_norm()

    for j in range(6):
        hidden(j)

    def products2(k):
        chip = (x + (0, 1, 2, -1)[k] + NX) % NX
        res = down(chip, slice(0, 2 * BLK))
        snd2[k] = res[:, OTHER].astype(BF)
        second.pair(k).start()
        mine[k] = res[:, OWN]

    def both(k):
        second.pair(k).wait_recv()
        return mine[k] + pre2[k].astype(F32)

    products2(2)
    products2(1)
    second.far(both(2))
    products2(3)
    second.near_right(both(1))
    products2(0)
    second.near_left(both(3))
    tot[0] = both(0)
    for q in SEQS:
        second.through(q)
    for q in SEQS:
        rows = pl.ds(SEQ * q, SEQ)
        out[rows, :] = (ambuf[t, rows, :].astype(F32) + 0.5 * (second.total(q) * dsc[...])).astype(BF)

    for ref, k in ((pall.at[0, pl.ds(0, 31 * 64), :], 0), (gbuf.at[pl.ds(0, 124 * 16), :], 1), (dbuf.at[pl.ds(0, 62 * 176), :], 2)):
        pltpu.make_async_remote_copy(
            src_ref=ref, dst_ref=ref, send_sem=psend.at[k], recv_sem=precv.at[0, 0], device_id={"fs": neighbour[0], "tp": t}
        ).wait_send()
    for ring in (ag1, sag, pag, gather):
        ring.done()
    first.done()
    second.done()


def body(
    stream, gain_first, gain_mixer, gain_second, gate_weight, gate_scale, up_weight, up_scale,
    down_weight, down_scale, pool_in_weight, pool_in_scale, pool_out_weight, pool_out_scale,
):
    def line(v):
        return v.reshape(1, -1)

    vmem = pl.BlockSpec(memory_space=pltpu.VMEM)
    V = pltpu.VMEM
    sem = pltpu.SemaphoreType.DMA
    exchange = [V((4, ROWS, BLK), BF), V((4, ROWS, BLK), BF), V((3, ROWS, BLK), BF), V((3, ROWS, BLK), BF)]
    ring_sems = [sem((2,)), sem((14,))]
    return pl.pallas_call(
        kernel,
        out_shape=jax.ShapeDtypeStruct((ROWS, BLK), BF),
        in_specs=[vmem] * 14,
        out_specs=vmem,
        scratch_shapes=[
            V((D, GUW), BF),
            V((32 * DH, 128), BF),
            V((NX, 768, 2 * BLK), BF),
            V((8, D, 128), BF),
            V((8, 16, 384), F32),
            V((D, 512), BF),
            V((512, D), BF),
            V((8, ROWS, BLK), BF),
            V((8, ROWS, BLK), BF),
            V((ROWS, D), BF),
            V((8, ROWS, BLK), BF),
            V((ROWS, 768), BF),
            V((ROWS, 128), F32),
            V((ROWS, 128), F32),
            V((ROWS, 512), F32),
            V((ROWS, 512), BF),
            *exchange,
            *exchange,
            V((4, ROWS, BLK), F32),
            V((4, ROWS, BLK), F32),
            V((1, FB), F32), V((1, FB), F32),
            sem((3,)), sem((7, 32)),
            *ring_sems, sem((2,)), sem((42,)), *ring_sems, *ring_sems,
            sem((2,)), sem((22,)), sem((2,)), sem((22,)),
        ],
        compiler_params=pltpu.CompilerParams(
            collective_id=0, has_side_effects=True, vmem_limit_bytes=60 * 1024 * 1024
        ),
    )(
        stream, line(gain_first), line(gain_mixer), line(gain_second), gate_weight, gate_scale, up_weight,
        up_scale, down_weight.T, line(down_scale), pool_in_weight, line(pool_in_scale), pool_out_weight,
        line(pool_out_scale),
    )


def solution(mesh):
    placed = (
        P("fs", "tp"), P(), P(), P(), P("fs", "tp"), P("tp"), P("fs", "tp"), P("tp"), P("tp", "fs"), P("tp"),
        P("fs", "tp"), P("tp"), P("tp", "fs"), P("tp"),
    )
    return jax.shard_map(body, mesh=mesh, in_specs=placed, out_specs=P("fs", "tp"), check_vma=False)
```

```python
import random

import jax
import jax.numpy as jnp
from jax import lax
from jax.experimental import pallas as pl
from jax.experimental.pallas import tpu as pltpu
from jax.sharding import PartitionSpec as P

SEQ = 128
EPS = 1e-06
WINDOWS = (2, 4, 8, 16)
NZ, NY, NX = 8, 4, 4
ROWS = 384
HALF = ROWS // 2
D = 2048
BLK = 256
FB = 704
GUW = 2 * FB
DH = FB // 2
BF = jnp.bfloat16
F32 = jnp.float32

SIZES = (0.36, 1, 1, 1, 1, 1, 1)
RANKS = (-1, 0, 0, 0, 0, 1, 1)
PIECES_G = (1, 2, 3, 4)
PIECES_D = (5, 6)
PLAN = (4.0, 10186, 1.0)
G_LATE, D_LATE = 1.0, 0.5


def moved(o, d):
    z, y = o
    if d == 0:
        return z, (y + 1) % NY
    if d == 1:
        return z, (y - 1) % NY
    return (z + (1 if d == 2 else -1)) % NZ, y


def broadcast_plan(lag=PLAN[0], seed=PLAN[1], noise=PLAN[2]):
    rng = random.Random(seed)
    count = len(SIZES)
    has = [{(0, 0): 0.0} for _ in range(count)]
    free = [0.0] * 4
    plan = []
    while len(plan) < count * (NZ * NY - 1):
        best = None
        for d in range(4):
            found = []
            for s in range(count):
                for o, t in has[s].items():
                    q = moved(o, d)
                    if q not in has[s]:
                        found.append((max(free[d], t), s, o, q))
            if found:
                first = min(c[0] for c in found)
                if best is None or first < best[0]:
                    best = (first, d, [c for c in found if c[0] <= first + 1e-9])
        _, d, found = best

        def key(c):
            onward = sum(moved(c[3], e) not in has[c[1]] for e in range(4))
            return RANKS[c[1]] * 1.5 - noise * rng.random() * 4 - onward * 0.5 + len(has[c[1]]) * 0.02

        start, s, o, q = min(found, key=key)
        has[s][q] = start + SIZES[s] + lag
        free[d] = start + SIZES[s]
        plan.append((start, d, s, o))
    return plan, has


def kernel(
    stream, gain1, gainm, gain2, gw, gsc1, uw, usc1, dw, dsc, iw, isc, ow, osc,
    out,
    gbuf, dbuf, dfull, pall, sall, infull, outfull, xall1, xall2, nbuf, ambuf, hid, ssacc, rst, pacc, pooled,
    snd1, pre1, sr1, rr1, snd2, pre2, sr2, rr2, mine, tot,
    gsc, usc, psend, precv, a1s, a1r, a2s, a2r, pas, par, sas, sar, r1s, r1r, r2s, r2r,
):
    f, t = lax.axis_index("fs"), lax.axis_index("tp")
    z, y = f // NY, f % NY
    x, c = t // 2, t % 2
    oc = 1 - c

    def at_f(dz, dy):
        return ((z + dz + NZ) % NZ) * NY + (y + dy + NY) % NY

    def at_t(dx, core):
        return ((x + dx + NX) % NX) * 2 + core

    neighbour = [at_f(0, 1), at_f(0, -1), at_f(1, 0), at_f(-1, 0)]
    right, left, twin = at_t(1, c), at_t(-1, c), at_t(0, oc)

    barrier = pltpu.get_barrier_semaphore()
    for nf in neighbour:
        pl.semaphore_signal(barrier, inc=1, device_id={"fs": nf, "tp": t})
    for nt in (right, left, twin):
        pl.semaphore_signal(barrier, inc=1, device_id={"fs": f, "tp": nt})

    prow = pl.ds(pl.multiple_of(f * 64, 64), 64)
    pall[t, prow, :] = jnp.concatenate([iw[...], ow[...]], axis=1).astype(BF)
    for j in range(5):
        gbuf[prow, 256 * j : 256 * j + 128] = gw[:, 128 * j : 128 * j + 128].astype(BF)
        gbuf[prow, 256 * j + 128 : 256 * j + 256] = uw[:, 128 * j : 128 * j + 128].astype(BF)
    gbuf[prow, 1280:1408] = jnp.concatenate([gw[:, 640:704], uw[:, 640:704]], axis=1).astype(BF)
    down_rows = jnp.transpose(dw[...])
    dbuf[pl.ds(pl.multiple_of(f * DH, 32), DH), :] = jnp.concatenate([down_rows[0:DH, :], down_rows[DH:FB, :]], axis=1).astype(BF)
    xall1[t] = stream[...]
    sall[t] = jnp.concatenate(
        [jnp.broadcast_to(osc[...], (16, 256)), jnp.broadcast_to(isc[...], (16, 64)), jnp.zeros((16, 64), F32)], axis=1
    )
    gsc[...] = gsc1[...].reshape(1, FB)
    usc[...] = usc1[...].reshape(1, FB)
    pl.semaphore_wait(barrier, 7)

    def piece(s, owner):
        if s == 0:
            return pall.at[t, pl.ds(pl.multiple_of(owner * 64, 64), 64), :]
        if s in PIECES_G:
            return gbuf.at[pl.ds(pl.multiple_of(owner * 64 + 16 * (s - 1), 16), 16), :]
        return dbuf.at[pl.ds(pl.multiple_of(owner * DH + 176 * (s - 5), 16), 176), :]

    def owner_of(o):
        return at_f(-o[0], -o[1])

    arrived = set()

    def ensure(s, o):
        if o == (0, 0) or (s, o) in arrived:
            return
        arrived.add((s, o))
        ref = piece(s, owner_of(o))
        pltpu.make_async_remote_copy(
            src_ref=ref, dst_ref=ref, send_sem=psend.at[0], recv_sem=precv.at[s, o[0] * NY + o[1]],
            device_id={"fs": neighbour[0], "tp": t},
        ).wait_recv()

    def send_piece(d, s, o):
        ensure(s, o)
        q = moved(o, d)
        ref = piece(s, owner_of(o))
        pltpu.make_async_remote_copy(
            src_ref=ref, dst_ref=ref, send_sem=psend.at[0 if s == 0 else 1 if s in PIECES_G else 2],
            recv_sem=precv.at[s, q[0] * NY + q[1]], device_id={"fs": neighbour[d], "tp": t},
        ).start()

    class Ring:
        def __init__(self, part, whole, ssem, rsem, base=0):
            self.part, self.whole, self.ssem, self.rsem, self.base = part, whole, ssem, rsem, base

        def copy(self, ref, to, rs):
            return pltpu.make_async_remote_copy(
                src_ref=ref, dst_ref=ref, send_sem=self.ssem.at[1 if rs >= 6 else 0], recv_sem=self.rsem.at[self.base + rs],
                device_id={"fs": f, "tp": to},
            )

        def start(self):
            me = t
            self.copy(self.part(me, 0), right, 0).start()
            self.copy(self.part(me, 1), left, 3).start()
            self.copy(self.part(me, 1), right, 1).start()
            self.copy(self.part(me, 0), left, 2).start()
            self.copy(self.part(me, 0), twin, 6).start()
            self.copy(self.part(me, 1), twin, 7).start()

        def block(self, k, core):
            return at_t((-1, -1, 1, 1, 2, 2, 0, 0)[k], core), k % 2

        def got(self, k, share=True):
            ref = self.part(*self.block(k, c))
            self.copy(ref, twin, k).wait_recv()
            if k == 0:
                self.copy(ref, right, 4).start()
            if k == 3:
                self.copy(ref, left, 5).start()
            if share:
                self.copy(ref, twin, 8 + k).start()

        def got_twin(self, k):
            ref = self.part(*self.block(k, oc))
            self.copy(ref, twin, 8 + k if k < 6 else k).wait_recv()

        def done(self):
            pltpu.make_async_remote_copy(
                src_ref=self.whole(3), dst_ref=self.whole(3), send_sem=self.ssem.at[0], recv_sem=self.rsem.at[0],
                device_id={"fs": f, "tp": twin},
            ).wait_send()
            pltpu.make_async_remote_copy(
                src_ref=self.whole(4), dst_ref=self.whole(4), send_sem=self.ssem.at[1], recv_sem=self.rsem.at[0],
                device_id={"fs": f, "tp": twin},
            ).wait_send()

    def halves(buf, size):
        return (
            lambda b, h: buf.at[b, pl.ds(h * (size // 2), size // 2), :],
            lambda n: buf.at[pl.ds(0, n)],
        )

    ag1 = Ring(*halves(xall1, ROWS), a1s, a1r)
    pag = Ring(*halves(pall, D), pas, par)
    sag = Ring(*halves(sall, 16), sas, sar)
    sag.part = lambda b, h: sall.at[b, pl.ds(h * 8, 8), :]

    def norm_block(b, src, gain, first):
        v = src[b].astype(F32)
        sq = v * v
        sq = sq[:, :128] + sq[:, 128:]
        ssacc[...] = sq if first else ssacc[...] + sq
        return (v * gain[:, b * BLK : (b + 1) * BLK]).astype(BF)

    def finish_norm():
        mean = jnp.sum(ssacc[...], axis=1, keepdims=True) * (1.0 / D)
        rst[...] = jnp.broadcast_to(lax.rsqrt(mean + EPS), (ROWS, 128))

    def norm1(b):
        nbuf[:, b * BLK : (b + 1) * BLK] = norm_block(b, xall1, gain1, b == 0)

    def hidden(j, at=0, size=ROWS):
        rows = slice(at, at + size)
        r = rst[rows, :]
        if j < 5:
            acc = jnp.dot(nbuf[rows, :], gbuf[:, 256 * j : 256 * j + 256], preferred_element_type=F32)
            g = acc[:, :128] * r * gsc[:, 128 * j : 128 * j + 128]
            u = acc[:, 128:] * r * usc[:, 128 * j : 128 * j + 128]
            hid[rows, 128 * j : 128 * j + 128] = (g / (1.0 + jnp.exp(-g)) * u).astype(BF)
        else:
            acc = jnp.dot(nbuf[rows, :], gbuf[:, 1280:1408], preferred_element_type=F32)
            scale = jnp.concatenate([gsc[:, 640:704], usc[:, 640:704]], axis=1)
            v = acc * r * scale
            u = pltpu.roll(v, 64, 1)
            h = v / (1.0 + jnp.exp(-v)) * u
            lane = lax.broadcasted_iota(jnp.int32, h.shape, 1)
            hid[rows, 640:768] = jnp.where(lane < 64, h, 0.0).astype(BF)

    def unpack_down(b):
        side = (b + c) % 2
        for pair in range(2):
            one = dbuf[pl.ds(pl.multiple_of((4 * b + 2 * pair) * DH, 32), DH), :]
            two = dbuf[pl.ds(pl.multiple_of((4 * b + 2 * pair + 1) * DH, 32), DH), :]
            cols = pl.ds(pl.multiple_of(side * BLK + 128 * pair, 128), 128)
            dfull[b // 2, 0:DH, cols] = jnp.concatenate([one[:, :64], two[:, :64]], axis=1)
            dfull[b // 2, DH:FB, cols] = jnp.concatenate([one[:, 64:], two[:, 64:]], axis=1)

    def unpack_in(k):
        rows = pl.ds(256 * k, 256)
        for i in range(NX):
            infull[rows, 128 * i : 128 * i + 128] = jnp.concatenate(
                [pall[2 * i, rows, :][:, :64], pall[2 * i + 1, rows, :][:, :64]], axis=1
            )

    def unpack_out(b):
        for i in range(16):
            outfull[64 * b : 64 * b + 64, 128 * i : 128 * i + 128] = jnp.concatenate(
                [pall[b, 128 * i : 128 * i + 64, :][:, 64:], pall[b, 128 * i + 64 : 128 * i + 128, :][:, 64:]], axis=1
            )

    def down(chip, cols):
        return jnp.dot(hid[...], dfull[chip, :, cols], preferred_element_type=F32)

    OWN, OTHER = slice(0, BLK), slice(BLK, 2 * BLK)

    SEQS = range(ROWS // SEQ)

    class Sum:
        def __init__(self, snd, pre, sr, rr, ss, rs):
            self.snd, self.pre, self.sr, self.rr, self.ss, self.rs = snd, pre, sr, rr, ss, rs

        def pair(self, k):
            return pltpu.make_async_remote_copy(
                src_ref=self.snd.at[k], dst_ref=self.pre.at[k], send_sem=self.ss.at[0], recv_sem=self.rs.at[k],
                device_id={"fs": f, "tp": twin},
            )

        def half(self, q, h):
            return pl.ds(SEQ * q + h * (SEQ // 2), SEQ // 2)

        def hop(self, q, src, slot, h, sem, to):
            rows = self.half(q, h)
            return pltpu.make_async_remote_copy(
                src_ref=self.sr.at[src, rows, :], dst_ref=self.rr.at[slot, rows, :], send_sem=self.ss.at[1],
                recv_sem=self.rs.at[4 + 6 * q + sem], device_id={"fs": f, "tp": to},
            )

        def far(self, total):
            self.sr[2] = total.astype(BF)
            for q in SEQS:
                self.hop(q, 2, 2, 0, 0, right).start()
                self.hop(q, 2, 2, 1, 1, left).start()

        def near_right(self, total):
            tot[1] = total
            for q in SEQS:
                rows = self.half(q, 1)
                self.sr[1, rows, :] = tot[1, rows, :].astype(BF)
                self.hop(q, 1, 0, 1, 2, right).start()

        def near_left(self, total):
            tot[3] = total
            for q in SEQS:
                rows = self.half(q, 0)
                self.sr[0, rows, :] = tot[3, rows, :].astype(BF)
                self.hop(q, 0, 1, 0, 3, left).start()

        def through(self, q):
            rows = self.half(q, 0)
            self.hop(q, 2, 2, 0, 0, right).wait_recv()
            self.sr[1, rows, :] = (tot[1, rows, :] + self.rr[2, rows, :].astype(F32)).astype(BF)
            self.hop(q, 1, 0, 0, 4, right).start()
            rows = self.half(q, 1)
            self.hop(q, 2, 2, 1, 1, left).wait_recv()
            self.sr[0, rows, :] = (tot[3, rows, :] + self.rr[2, rows, :].astype(F32)).astype(BF)
            self.hop(q, 0, 1, 1, 5, left).start()

        def total(self, q):
            self.hop(q, 1, 0, 1, 2, right).wait_recv()
            self.hop(q, 0, 1, 0, 3, left).wait_recv()
            self.hop(q, 1, 0, 0, 4, right).wait_recv()
            self.hop(q, 0, 1, 1, 5, left).wait_recv()
            rows = pl.ds(SEQ * q, SEQ)
            return tot[0, rows, :] + self.rr[0, rows, :].astype(F32) + self.rr[1, rows, :].astype(F32)

        def done(self):
            for ref, k in ((self.snd.at[pl.ds(0, 4)], 0), (self.sr.at[pl.ds(0, 3)], 1)):
                pltpu.make_async_remote_copy(
                    src_ref=ref, dst_ref=ref, send_sem=self.ss.at[k], recv_sem=self.rs.at[0],
                    device_id={"fs": f, "tp": twin},
                ).wait_send()

    first = Sum(snd1, pre1, sr1, rr1, r1s, r1r)
    second = Sum(snd2, pre2, sr2, rr2, r2s, r2r)

    plan, has = broadcast_plan()
    events = []

    def when(time, fn):
        events.append((time, len(events), fn))

    for start, d, s, o in plan:
        when(start, lambda d=d, s=s, o=o: send_piece(d, s, o))

    when(1.5, ag1.start)
    when(1.6, sag.start)
    for k, time in ((0, 5.5), (3, 5.5), (1, 8.5), (2, 8.5), (4, 11.0), (5, 11.0)):
        when(time, lambda k=k: ag1.got(k))
        when(time + 0.01, lambda k=k: sag.got(k))

    def twin1():
        for k in range(8):
            ag1.got_twin(k)
            sag.got_twin(k)

    when(13.0, twin1)
    for b in range(8):
        when(13.2 + 0.6 * b, lambda b=b: norm1(b))
    when(18.2, finish_norm)

    p_done = max(has[0].values())

    def pool_ring():
        for o in has[0]:
            ensure(0, o)
        pag.start()

    when(p_done, pool_ring)
    for k, time in ((0, 8.5), (3, 8.5), (1, 15.0), (2, 15.0), (4, 22.5), (5, 22.5)):
        when(p_done + time, lambda k=k: pag.got(k))

    def twin_pool():
        for k in range(8):
            pag.got_twin(k)


    g_done = max(max(has[s].values()) for s in PIECES_G)

    def gates():
        for s in PIECES_G:
            for o in has[s]:
                ensure(s, o)

    when(g_done + G_LATE, gates)

    def hidden_part(js):
        for j in js:
            hidden(j)

    when(g_done + G_LATE + 0.1, lambda: hidden_part((0, 1, 2)))
    when(g_done + G_LATE + 1.9, lambda: hidden_part((3, 4, 5)))

    def plane(oz):
        for s in PIECES_D:
            for oy in range(NY):
                ensure(s, (oz, oy))
        unpack_down((z - oz + NZ) % NZ)

    def clear_down():
        dfull[:, FB:768, :] = jnp.zeros((NX, 768 - FB, 2 * BLK), BF)

    when(0.5, clear_down)
    ready = {oz: max(has[s][oz, oy] for s in PIECES_D for oy in range(NY)) for oz in range(NZ)}
    even, odd = (sorted(range(e, NZ, 2), key=lambda oz: ready[oz]) for e in (0, 1))
    turn = (z + c) % 2

    def products(i):
        one, two = (z - even[i] + NZ) % NZ, (z - odd[i] + NZ) % NZ
        for_twin = one * turn + two * (1 - turn)
        own = two * turn + one * (1 - turn)
        theirs, ours = down(for_twin // 2, OTHER), down(own // 2, OWN)
        snd1[i] = theirs.astype(BF)
        mine[i] = ours
        first.pair(i).start()

    def combine(i):
        one, two = (z - even[i] + NZ) % NZ, (z - odd[i] + NZ) % NZ
        own = two * turn + one * (1 - turn)
        away = (own // 2 - x + NX) % NX
        first.pair(i).wait_recv()
        mine[i] = mine[i] + pre1[i].astype(F32)

        @pl.when(away == 2)
        def _():
            first.far(mine[i])

        @pl.when(away == 1)
        def _():
            first.near_right(mine[i])

        @pl.when(away == 3)
        def _():
            first.near_left(mine[i])

        @pl.when(away == 0)
        def _():
            tot[0] = mine[i]

    hid_done = g_done + G_LATE + 3.6
    for oz in range(NZ):
        when(ready[oz] + D_LATE, lambda oz=oz: plane(oz))
    for i in range(4):
        at = max(hid_done + 1.0 * i, max(ready[even[i]], ready[odd[i]]) + D_LATE + 0.01)
        when(at, lambda i=i: products(i))
        when(at + 1.6, lambda i=i: combine(i))

    def pool_weights():
        twin_pool()
        for b in range(8):
            unpack_in(b)
            unpack_out(b)

    when(at + 0.2, pool_weights)

    for _, _, fn in sorted(events, key=lambda e: e[:2]):
        fn()

    for q in SEQS:
        first.through(q)
    gathers = []
    for q in SEQS:
        gather = Ring(
            lambda b, h, q=q: xall2.at[b, pl.ds(SEQ * q + h * (SEQ // 2), SEQ // 2), :],
            lambda n: xall2.at[pl.ds(0, n)], a2s, a2r, 14 * q,
        )
        gathers.append(gather)
        rows = pl.ds(SEQ * q, SEQ)
        xall2[t, rows, :] = (stream[rows, :].astype(F32) + 0.5 * (first.total(q) * dsc[...])).astype(BF)
        gather.start()

    def enter(b, start=False):
        v = xall2[b].astype(F32)
        sq = v * v
        sq = sq[:, :128] + sq[:, 128:]
        at = pl.multiple_of(b * BLK, BLK)
        w = (v * gainm[:, pl.ds(at, BLK)]).astype(BF)
        part = jnp.dot(w, infull[pl.ds(at, BLK), :], preferred_element_type=F32)
        ssacc[...] = sq if start else ssacc[...] + sq
        pacc[...] = part if start else pacc[...] + part

    enter(t, True)
    for q in SEQS:
        for k in (0, 3):
            gathers[q].got(k)
    for q in SEQS:
        gathers[q].got_twin(6)
        gathers[q].got_twin(7)
    enter(twin)
    for q in SEQS:
        for k in (1, 2):
            gathers[q].got(k)
    enter(left)
    enter(right)
    for q in SEQS:
        for k in (0, 1, 2, 3):
            gathers[q].got_twin(k)
    enter(at_t(-1, oc))
    enter(at_t(1, oc))
    for q in SEQS:
        for k in (4, 5):
            gathers[q].got(k)
    enter(at_t(2, c))
    for q in SEQS:
        for k in (4, 5):
            gathers[q].got_twin(k)
    enter(at_t(2, oc))
    finish_norm()
    row = lax.broadcasted_iota(jnp.int32, (SEQ, SEQ), 0)
    col = lax.broadcasted_iota(jnp.int32, (SEQ, SEQ), 1)
    for g, window in enumerate(WINDOWS):
        low = jnp.maximum(row - window // 2, 0)
        high = jnp.minimum(row + window - window // 2, SEQ)
        band = jnp.where((col >= low) & (col < high), 1.0, 0.0).astype(BF)
        count = (high - low).astype(F32)
        scale = jnp.concatenate([sall[2 * g, 0:1, 256:320], sall[2 * g + 1, 0:1, 256:320]], axis=1)
        cols = slice(128 * g, 128 * g + 128)
        value = (pacc[:, cols] * rst[...] * scale).astype(BF)
        side = jnp.concatenate([value[SEQ * q : SEQ * q + SEQ] for q in SEQS], axis=1)
        whole = jnp.dot(band, side, preferred_element_type=F32)
        for q in SEQS:
            rows = slice(SEQ * q, SEQ * q + SEQ)
            mean = whole[:, SEQ * q : SEQ * q + SEQ] / count
            pooled[rows, cols] = (mean - value[rows].astype(F32)).astype(BF)
    for b in range(8):
        cols = slice(b * BLK, (b + 1) * BLK)
        mix = jnp.dot(pooled[...], outfull[:, cols], preferred_element_type=F32)
        v = (xall2[b].astype(F32) + mix * sall[b, 0:1, 0:256]).astype(BF)
        ambuf[b] = v
        nbuf[:, cols] = norm_block(b, ambuf, gain2, b == 0)
    finish_norm()

    for j in range(6):
        hidden(j)

    def products2(k):
        chip = (x + (0, 1, 2, -1)[k] + NX) % NX
        res = down(chip, slice(0, 2 * BLK))
        snd2[k] = res[:, OTHER].astype(BF)
        second.pair(k).start()
        mine[k] = res[:, OWN]

    def both(k):
        second.pair(k).wait_recv()
        return mine[k] + pre2[k].astype(F32)

    products2(2)
    products2(1)
    products2(3)
    second.far(both(2))
    second.near_right(both(1))
    products2(0)
    second.near_left(both(3))
    tot[0] = both(0)
    for q in SEQS:
        second.through(q)
    for q in SEQS:
        rows = pl.ds(SEQ * q, SEQ)
        out[rows, :] = (ambuf[t, rows, :].astype(F32) + 0.5 * (second.total(q) * dsc[...])).astype(BF)

    for ref, k in ((pall.at[0, pl.ds(0, 31 * 64), :], 0), (gbuf.at[pl.ds(0, 124 * 16), :], 1), (dbuf.at[pl.ds(0, 62 * 176), :], 2)):
        pltpu.make_async_remote_copy(
            src_ref=ref, dst_ref=ref, send_sem=psend.at[k], recv_sem=precv.at[0, 0], device_id={"fs": neighbour[0], "tp": t}
        ).wait_send()
    for ring in (ag1, sag, pag, gather):
        ring.done()
    first.done()
    second.done()


def body(
    stream, gain_first, gain_mixer, gain_second, gate_weight, gate_scale, up_weight, up_scale,
    down_weight, down_scale, pool_in_weight, pool_in_scale, pool_out_weight, pool_out_scale,
):
    def line(v):
        return v.reshape(1, -1)

    vmem = pl.BlockSpec(memory_space=pltpu.VMEM)
    V = pltpu.VMEM
    sem = pltpu.SemaphoreType.DMA
    exchange = [V((4, ROWS, BLK), BF), V((4, ROWS, BLK), BF), V((3, ROWS, BLK), BF), V((3, ROWS, BLK), BF)]
    ring_sems = [sem((2,)), sem((14,))]
    return pl.pallas_call(
        kernel,
        out_shape=jax.ShapeDtypeStruct((ROWS, BLK), BF),
        in_specs=[vmem] * 14,
        out_specs=vmem,
        scratch_shapes=[
            V((D, GUW), BF),
            V((32 * DH, 128), BF),
            V((NX, 768, 2 * BLK), BF),
            V((8, D, 128), BF),
            V((8, 16, 384), F32),
            V((D, 512), BF),
            V((512, D), BF),
            V((8, ROWS, BLK), BF),
            V((8, ROWS, BLK), BF),
            V((ROWS, D), BF),
            V((8, ROWS, BLK), BF),
            V((ROWS, 768), BF),
            V((ROWS, 128), F32),
            V((ROWS, 128), F32),
            V((ROWS, 512), F32),
            V((ROWS, 512), BF),
            *exchange,
            *exchange,
            V((4, ROWS, BLK), F32),
            V((4, ROWS, BLK), F32),
            V((1, FB), F32), V((1, FB), F32),
            sem((3,)), sem((7, 32)),
            *ring_sems, sem((2,)), sem((42,)), *ring_sems, *ring_sems,
            sem((2,)), sem((22,)), sem((2,)), sem((22,)),
        ],
        compiler_params=pltpu.CompilerParams(
            collective_id=0, has_side_effects=True, vmem_limit_bytes=60 * 1024 * 1024
        ),
    )(
        stream, line(gain_first), line(gain_mixer), line(gain_second), gate_weight, gate_scale, up_weight,
        up_scale, down_weight.T, line(down_scale), pool_in_weight, line(pool_in_scale), pool_out_weight,
        line(pool_out_scale),
    )


def solution(mesh):
    placed = (
        P("fs", "tp"), P(), P(), P(), P("fs", "tp"), P("tp"), P("fs", "tp"), P("tp"), P("tp", "fs"), P("tp"),
        P("fs", "tp"), P("tp"), P("tp", "fs"), P("tp"),
    )
    return jax.shard_map(body, mesh=mesh, in_specs=placed, out_specs=P("fs", "tp"), check_vma=False)
```

```python
import random

import jax
import jax.numpy as jnp
from jax import lax
from jax.experimental import pallas as pl
from jax.experimental.pallas import tpu as pltpu
from jax.sharding import PartitionSpec as P

SEQ = 128
EPS = 1e-06
WINDOWS = (2, 4, 8, 16)
NZ, NY, NX = 8, 4, 4
ROWS = 384
HALF = ROWS // 2
D = 2048
BLK = 256
FB = 704
GUW = 2 * FB
DH = FB // 2
BF = jnp.bfloat16
F32 = jnp.float32

SIZES = (0.36, 1, 1, 1, 1, 1, 1)
RANKS = (-1, 0, 0, 0, 0, 1, 1)
PIECES_G = (1, 2, 3, 4)
PIECES_D = (5, 6)
PLAN = (4.0, 10186, 1.0)
G_LATE, D_LATE = 1.0, 0.5


def moved(o, d):
    z, y = o
    if d == 0:
        return z, (y + 1) % NY
    if d == 1:
        return z, (y - 1) % NY
    return (z + (1 if d == 2 else -1)) % NZ, y


def broadcast_plan(lag=PLAN[0], seed=PLAN[1], noise=PLAN[2]):
    rng = random.Random(seed)
    count = len(SIZES)
    has = [{(0, 0): 0.0} for _ in range(count)]
    free = [0.0] * 4
    plan = []
    while len(plan) < count * (NZ * NY - 1):
        best = None
        for d in range(4):
            found = []
            for s in range(count):
                for o, t in has[s].items():
                    q = moved(o, d)
                    if q not in has[s]:
                        found.append((max(free[d], t), s, o, q))
            if found:
                first = min(c[0] for c in found)
                if best is None or first < best[0]:
                    best = (first, d, [c for c in found if c[0] <= first + 1e-9])
        _, d, found = best

        def key(c):
            onward = sum(moved(c[3], e) not in has[c[1]] for e in range(4))
            return RANKS[c[1]] * 1.5 - noise * rng.random() * 4 - onward * 0.5 + len(has[c[1]]) * 0.02

        start, s, o, q = min(found, key=key)
        has[s][q] = start + SIZES[s] + lag
        free[d] = start + SIZES[s]
        plan.append((start, d, s, o))
    return plan, has


def kernel(
    *refs,
):
    hbm, out, rest = refs[:14], refs[14], refs[15:]
    (
        gbuf, dbuf, dfull, pall, sall, infull, outfull, xall1, xall2, nbuf, ambuf, hid, ssacc, rst, pacc, pooled,
        snd1, pre1, sr1, rr1, snd2, pre2, sr2, rr2, mine, tot,
        gsc, usc, psend, precv, a1s, a1r, a2s, a2r, pas, par, sas, sar, r1s, r1r, r2s, r2r,
        gain1, gainm, gain2, gw, gsc1, uw, usc1, dw, dsc, iw, isc, ow, osc, insem,
    ) = rest
    f, t = lax.axis_index("fs"), lax.axis_index("tp")
    z, y = f // NY, f % NY
    x, c = t // 2, t % 2
    oc = 1 - c

    def at_f(dz, dy):
        return ((z + dz + NZ) % NZ) * NY + (y + dy + NY) % NY

    def at_t(dx, core):
        return ((x + dx + NX) % NX) * 2 + core

    inputs = [
        pltpu.make_async_copy(src, dst, insem.at[i])
        for i, (src, dst) in enumerate(
            zip(hbm, (xall1.at[t], gain1, gainm, gain2, gw, gsc1, uw, usc1, dw, dsc, iw, isc, ow, osc))
        )
    ]
    for i in (10, 12, 4, 6, 8, 0, 1, 2, 3, 5, 7, 9, 11, 13):
        inputs[i].start()

    neighbour = [at_f(0, 1), at_f(0, -1), at_f(1, 0), at_f(-1, 0)]
    right, left, twin = at_t(1, c), at_t(-1, c), at_t(0, oc)

    barrier = pltpu.get_barrier_semaphore()
    for nf in neighbour:
        pl.semaphore_signal(barrier, inc=1, device_id={"fs": nf, "tp": t})
    for nt in (right, left, twin):
        pl.semaphore_signal(barrier, inc=1, device_id={"fs": f, "tp": nt})

    for copy in inputs:
        copy.wait()
    prow = pl.ds(pl.multiple_of(f * 64, 64), 64)
    pall[t, prow, :] = jnp.concatenate([iw[...], ow[...]], axis=1).astype(BF)
    for j in range(5):
        gbuf[prow, 256 * j : 256 * j + 128] = gw[:, 128 * j : 128 * j + 128].astype(BF)
        gbuf[prow, 256 * j + 128 : 256 * j + 256] = uw[:, 128 * j : 128 * j + 128].astype(BF)
    gbuf[prow, 1280:1408] = jnp.concatenate([gw[:, 640:704], uw[:, 640:704]], axis=1).astype(BF)
    down_rows = jnp.transpose(dw[...])
    dbuf[pl.ds(pl.multiple_of(f * DH, 32), DH), :] = jnp.concatenate([down_rows[0:DH, :], down_rows[DH:FB, :]], axis=1).astype(BF)
    sall[t] = jnp.concatenate(
        [jnp.broadcast_to(osc[...], (16, 256)), jnp.broadcast_to(isc[...], (16, 64)), jnp.zeros((16, 64), F32)], axis=1
    )
    gsc[...] = gsc1[...].reshape(1, FB)
    usc[...] = usc1[...].reshape(1, FB)
    pl.semaphore_wait(barrier, 7)

    def piece(s, owner):
        if s == 0:
            return pall.at[t, pl.ds(pl.multiple_of(owner * 64, 64), 64), :]
        if s in PIECES_G:
            return gbuf.at[pl.ds(pl.multiple_of(owner * 64 + 16 * (s - 1), 16), 16), :]
        return dbuf.at[pl.ds(pl.multiple_of(owner * DH + 176 * (s - 5), 16), 176), :]

    def owner_of(o):
        return at_f(-o[0], -o[1])

    arrived = set()

    def ensure(s, o):
        if o == (0, 0) or (s, o) in arrived:
            return
        arrived.add((s, o))
        ref = piece(s, owner_of(o))
        pltpu.make_async_remote_copy(
            src_ref=ref, dst_ref=ref, send_sem=psend.at[0], recv_sem=precv.at[s, o[0] * NY + o[1]],
            device_id={"fs": neighbour[0], "tp": t},
        ).wait_recv()

    def send_piece(d, s, o):
        ensure(s, o)
        q = moved(o, d)
        ref = piece(s, owner_of(o))
        pltpu.make_async_remote_copy(
            src_ref=ref, dst_ref=ref, send_sem=psend.at[0 if s == 0 else 1 if s in PIECES_G else 2],
            recv_sem=precv.at[s, q[0] * NY + q[1]], device_id={"fs": neighbour[d], "tp": t},
        ).start()

    class Ring:
        def __init__(self, part, whole, ssem, rsem, base=0):
            self.part, self.whole, self.ssem, self.rsem, self.base = part, whole, ssem, rsem, base

        def copy(self, ref, to, rs):
            return pltpu.make_async_remote_copy(
                src_ref=ref, dst_ref=ref, send_sem=self.ssem.at[1 if rs >= 6 else 0], recv_sem=self.rsem.at[self.base + rs],
                device_id={"fs": f, "tp": to},
            )

        def start(self):
            me = t
            self.copy(self.part(me, 0), right, 0).start()
            self.copy(self.part(me, 1), left, 3).start()
            self.copy(self.part(me, 1), right, 1).start()
            self.copy(self.part(me, 0), left, 2).start()
            self.copy(self.part(me, 0), twin, 6).start()
            self.copy(self.part(me, 1), twin, 7).start()

        def block(self, k, core):
            return at_t((-1, -1, 1, 1, 2, 2, 0, 0)[k], core), k % 2

        def got(self, k, share=True):
            ref = self.part(*self.block(k, c))
            self.copy(ref, twin, k).wait_recv()
            if k == 0:
                self.copy(ref, right, 4).start()
            if k == 3:
                self.copy(ref, left, 5).start()
            if share:
                self.copy(ref, twin, 8 + k).start()

        def got_twin(self, k):
            ref = self.part(*self.block(k, oc))
            self.copy(ref, twin, 8 + k if k < 6 else k).wait_recv()

        def done(self):
            pltpu.make_async_remote_copy(
                src_ref=self.whole(3), dst_ref=self.whole(3), send_sem=self.ssem.at[0], recv_sem=self.rsem.at[0],
                device_id={"fs": f, "tp": twin},
            ).wait_send()
            pltpu.make_async_remote_copy(
                src_ref=self.whole(4), dst_ref=self.whole(4), send_sem=self.ssem.at[1], recv_sem=self.rsem.at[0],
                device_id={"fs": f, "tp": twin},
            ).wait_send()

    def halves(buf, size):
        return (
            lambda b, h: buf.at[b, pl.ds(h * (size // 2), size // 2), :],
            lambda n: buf.at[pl.ds(0, n)],
        )

    ag1 = Ring(*halves(xall1, ROWS), a1s, a1r)
    pag = Ring(*halves(pall, D), pas, par)
    sag = Ring(*halves(sall, 16), sas, sar)
    sag.part = lambda b, h: sall.at[b, pl.ds(h * 8, 8), :]

    def norm_block(b, src, gain, first):
        v = src[b].astype(F32)
        sq = v * v
        sq = sq[:, :128] + sq[:, 128:]
        ssacc[...] = sq if first else ssacc[...] + sq
        return (v * gain[:, b * BLK : (b + 1) * BLK]).astype(BF)

    def finish_norm():
        mean = jnp.sum(ssacc[...], axis=1, keepdims=True) * (1.0 / D)
        rst[...] = jnp.broadcast_to(lax.rsqrt(mean + EPS), (ROWS, 128))

    def norm1(b):
        nbuf[:, b * BLK : (b + 1) * BLK] = norm_block(b, xall1, gain1, b == 0)

    def hidden(j, at=0, size=ROWS):
        rows = slice(at, at + size)
        r = rst[rows, :]
        if j < 5:
            acc = jnp.dot(nbuf[rows, :], gbuf[:, 256 * j : 256 * j + 256], preferred_element_type=F32)
            g = acc[:, :128] * r * gsc[:, 128 * j : 128 * j + 128]
            u = acc[:, 128:] * r * usc[:, 128 * j : 128 * j + 128]
            hid[rows, 128 * j : 128 * j + 128] = (g / (1.0 + jnp.exp(-g)) * u).astype(BF)
        else:
            acc = jnp.dot(nbuf[rows, :], gbuf[:, 1280:1408], preferred_element_type=F32)
            scale = jnp.concatenate([gsc[:, 640:704], usc[:, 640:704]], axis=1)
            v = acc * r * scale
            u = pltpu.roll(v, 64, 1)
            h = v / (1.0 + jnp.exp(-v)) * u
            lane = lax.broadcasted_iota(jnp.int32, h.shape, 1)
            hid[rows, 640:768] = jnp.where(lane < 64, h, 0.0).astype(BF)

    def unpack_down(b):
        side = (b + c) % 2
        for pair in range(2):
            one = dbuf[pl.ds(pl.multiple_of((4 * b + 2 * pair) * DH, 32), DH), :]
            two = dbuf[pl.ds(pl.multiple_of((4 * b + 2 * pair + 1) * DH, 32), DH), :]
            cols = pl.ds(pl.multiple_of(side * BLK + 128 * pair, 128), 128)
            dfull[b // 2, 0:DH, cols] = jnp.concatenate([one[:, :64], two[:, :64]], axis=1)
            dfull[b // 2, DH:FB, cols] = jnp.concatenate([one[:, 64:], two[:, 64:]], axis=1)

    def unpack_in(k):
        rows = pl.ds(256 * k, 256)
        for i in range(NX):
            infull[rows, 128 * i : 128 * i + 128] = jnp.concatenate(
                [pall[2 * i, rows, :][:, :64], pall[2 * i + 1, rows, :][:, :64]], axis=1
            )

    def unpack_out(b):
        for i in range(16):
            outfull[64 * b : 64 * b + 64, 128 * i : 128 * i + 128] = jnp.concatenate(
                [pall[b, 128 * i : 128 * i + 64, :][:, 64:], pall[b, 128 * i + 64 : 128 * i + 128, :][:, 64:]], axis=1
            )

    def down(chip, cols):
        return jnp.dot(hid[...], dfull[chip, :, cols], preferred_element_type=F32)

    OWN, OTHER = slice(0, BLK), slice(BLK, 2 * BLK)

    SEQS = range(ROWS // SEQ)

    class Sum:
        def __init__(self, snd, pre, sr, rr, ss, rs):
            self.snd, self.pre, self.sr, self.rr, self.ss, self.rs = snd, pre, sr, rr, ss, rs

        def pair(self, k):
            return pltpu.make_async_remote_copy(
                src_ref=self.snd.at[k], dst_ref=self.pre.at[k], send_sem=self.ss.at[0], recv_sem=self.rs.at[k],
                device_id={"fs": f, "tp": twin},
            )

        def half(self, q, h):
            return pl.ds(SEQ * q + h * (SEQ // 2), SEQ // 2)

        def hop(self, q, src, slot, h, sem, to):
            rows = self.half(q, h)
            return pltpu.make_async_remote_copy(
                src_ref=self.sr.at[src, rows, :], dst_ref=self.rr.at[slot, rows, :], send_sem=self.ss.at[1],
                recv_sem=self.rs.at[4 + 6 * q + sem], device_id={"fs": f, "tp": to},
            )

        def far(self, total):
            self.sr[2] = total.astype(BF)
            for q in SEQS:
                self.hop(q, 2, 2, 0, 0, right).start()
                self.hop(q, 2, 2, 1, 1, left).start()

        def near_right(self, total):
            tot[1] = total
            for q in SEQS:
                rows = self.half(q, 1)
                self.sr[1, rows, :] = tot[1, rows, :].astype(BF)
                self.hop(q, 1, 0, 1, 2, right).start()

        def near_left(self, total):
            tot[3] = total
            for q in SEQS:
                rows = self.half(q, 0)
                self.sr[0, rows, :] = tot[3, rows, :].astype(BF)
                self.hop(q, 0, 1, 0, 3, left).start()

        def through(self, q):
            rows = self.half(q, 0)
            self.hop(q, 2, 2, 0, 0, right).wait_recv()
            self.sr[1, rows, :] = (tot[1, rows, :] + self.rr[2, rows, :].astype(F32)).astype(BF)
            self.hop(q, 1, 0, 0, 4, right).start()
            rows = self.half(q, 1)
            self.hop(q, 2, 2, 1, 1, left).wait_recv()
            self.sr[0, rows, :] = (tot[3, rows, :] + self.rr[2, rows, :].astype(F32)).astype(BF)
            self.hop(q, 0, 1, 1, 5, left).start()

        def total(self, q):
            self.hop(q, 1, 0, 1, 2, right).wait_recv()
            self.hop(q, 0, 1, 0, 3, left).wait_recv()
            self.hop(q, 1, 0, 0, 4, right).wait_recv()
            self.hop(q, 0, 1, 1, 5, left).wait_recv()
            rows = pl.ds(SEQ * q, SEQ)
            return tot[0, rows, :] + self.rr[0, rows, :].astype(F32) + self.rr[1, rows, :].astype(F32)

        def done(self):
            for ref, k in ((self.snd.at[pl.ds(0, 4)], 0), (self.sr.at[pl.ds(0, 3)], 1)):
                pltpu.make_async_remote_copy(
                    src_ref=ref, dst_ref=ref, send_sem=self.ss.at[k], recv_sem=self.rs.at[0],
                    device_id={"fs": f, "tp": twin},
                ).wait_send()

    first = Sum(snd1, pre1, sr1, rr1, r1s, r1r)
    second = Sum(snd2, pre2, sr2, rr2, r2s, r2r)

    plan, has = broadcast_plan()
    events = []

    def when(time, fn):
        events.append((time, len(events), fn))

    for start, d, s, o in plan:
        when(start, lambda d=d, s=s, o=o: send_piece(d, s, o))

    when(1.5, ag1.start)
    when(1.6, sag.start)
    for k, time in ((0, 5.5), (3, 5.5), (1, 8.5), (2, 8.5), (4, 11.0), (5, 11.0)):
        when(time, lambda k=k: ag1.got(k))
        when(time + 0.01, lambda k=k: sag.got(k))

    def twin1():
        for k in range(8):
            ag1.got_twin(k)
            sag.got_twin(k)

    when(13.0, twin1)
    for b in range(8):
        when(13.2 + 0.6 * b, lambda b=b: norm1(b))
    when(18.2, finish_norm)

    p_done = max(has[0].values())

    def pool_ring():
        for o in has[0]:
            ensure(0, o)
        pag.start()

    when(p_done, pool_ring)
    for k, time in ((0, 8.5), (3, 8.5), (1, 15.0), (2, 15.0), (4, 22.5), (5, 22.5)):
        when(p_done + time, lambda k=k: pag.got(k))

    def twin_pool():
        for k in range(8):
            pag.got_twin(k)


    g_done = max(max(has[s].values()) for s in PIECES_G)

    def gates():
        for s in PIECES_G:
            for o in has[s]:
                ensure(s, o)

    when(g_done + G_LATE, gates)

    def hidden_part(js):
        for j in js:
            hidden(j)

    when(g_done + G_LATE + 0.1, lambda: hidden_part((0, 1, 2)))
    when(g_done + G_LATE + 1.9, lambda: hidden_part((3, 4, 5)))

    def plane(oz):
        for s in PIECES_D:
            for oy in range(NY):
                ensure(s, (oz, oy))
        unpack_down((z - oz + NZ) % NZ)

    def clear_down():
        dfull[:, FB:768, :] = jnp.zeros((NX, 768 - FB, 2 * BLK), BF)

    when(0.5, clear_down)
    ready = {oz: max(has[s][oz, oy] for s in PIECES_D for oy in range(NY)) for oz in range(NZ)}
    even, odd = (sorted(range(e, NZ, 2), key=lambda oz: ready[oz]) for e in (0, 1))
    turn = (z + c) % 2

    def products(i):
        one, two = (z - even[i] + NZ) % NZ, (z - odd[i] + NZ) % NZ
        for_twin = one * turn + two * (1 - turn)
        own = two * turn + one * (1 - turn)
        theirs, ours = down(for_twin // 2, OTHER), down(own // 2, OWN)
        snd1[i] = theirs.astype(BF)
        mine[i] = ours
        first.pair(i).start()

    def combine(i):
        one, two = (z - even[i] + NZ) % NZ, (z - odd[i] + NZ) % NZ
        own = two * turn + one * (1 - turn)
        away = (own // 2 - x + NX) % NX
        first.pair(i).wait_recv()
        mine[i] = mine[i] + pre1[i].astype(F32)

        @pl.when(away == 2)
        def _():
            first.far(mine[i])

        @pl.when(away == 1)
        def _():
            first.near_right(mine[i])

        @pl.when(away == 3)
        def _():
            first.near_left(mine[i])

        @pl.when(away == 0)
        def _():
            tot[0] = mine[i]

    hid_done = g_done + G_LATE + 3.6
    for oz in range(NZ):
        when(ready[oz] + D_LATE, lambda oz=oz: plane(oz))
    for i in range(4):
        at = max(hid_done + 1.0 * i, max(ready[even[i]], ready[odd[i]]) + D_LATE + 0.01)
        when(at, lambda i=i: products(i))
        when(at + 1.6, lambda i=i: combine(i))

    def pool_weights():
        twin_pool()
        for b in range(8):
            unpack_in(b)
            unpack_out(b)

    when(at + 0.2, pool_weights)

    for _, _, fn in sorted(events, key=lambda e: e[:2]):
        fn()

    for q in SEQS:
        first.through(q)
    gathers = []
    for q in SEQS:
        gather = Ring(
            lambda b, h, q=q: xall2.at[b, pl.ds(SEQ * q + h * (SEQ // 2), SEQ // 2), :],
            lambda n: xall2.at[pl.ds(0, n)], a2s, a2r, 14 * q,
        )
        gathers.append(gather)
        rows = pl.ds(SEQ * q, SEQ)
        xall2[t, rows, :] = (xall1[t, rows, :].astype(F32) + 0.5 * (first.total(q) * dsc[...])).astype(BF)
        gather.start()

    def enter(b, start=False):
        v = xall2[b].astype(F32)
        sq = v * v
        sq = sq[:, :128] + sq[:, 128:]
        at = pl.multiple_of(b * BLK, BLK)
        w = (v * gainm[:, pl.ds(at, BLK)]).astype(BF)
        part = jnp.dot(w, infull[pl.ds(at, BLK), :], preferred_element_type=F32)
        ssacc[...] = sq if start else ssacc[...] + sq
        pacc[...] = part if start else pacc[...] + part

    enter(t, True)
    for q in SEQS:
        for k in (0, 3):
            gathers[q].got(k)
    for q in SEQS:
        gathers[q].got_twin(6)
        gathers[q].got_twin(7)
    enter(twin)
    for q in SEQS:
        for k in (1, 2):
            gathers[q].got(k)
    enter(left)
    enter(right)
    for q in SEQS:
        for k in (0, 1, 2, 3):
            gathers[q].got_twin(k)
    enter(at_t(-1, oc))
    enter(at_t(1, oc))
    for q in SEQS:
        for k in (4, 5):
            gathers[q].got(k)
    enter(at_t(2, c))
    for q in SEQS:
        for k in (4, 5):
            gathers[q].got_twin(k)
    enter(at_t(2, oc))
    finish_norm()
    row = lax.broadcasted_iota(jnp.int32, (SEQ, SEQ), 0)
    col = lax.broadcasted_iota(jnp.int32, (SEQ, SEQ), 1)
    for g, window in enumerate(WINDOWS):
        low = jnp.maximum(row - window // 2, 0)
        high = jnp.minimum(row + window - window // 2, SEQ)
        band = jnp.where((col >= low) & (col < high), 1.0, 0.0).astype(BF)
        count = (high - low).astype(F32)
        scale = jnp.concatenate([sall[2 * g, 0:1, 256:320], sall[2 * g + 1, 0:1, 256:320]], axis=1)
        cols = slice(128 * g, 128 * g + 128)
        value = (pacc[:, cols] * rst[...] * scale).astype(BF)
        side = jnp.concatenate([value[SEQ * q : SEQ * q + SEQ] for q in SEQS], axis=1)
        whole = jnp.dot(band, side, preferred_element_type=F32)
        for q in SEQS:
            rows = slice(SEQ * q, SEQ * q + SEQ)
            mean = whole[:, SEQ * q : SEQ * q + SEQ] / count
            pooled[rows, cols] = (mean - value[rows].astype(F32)).astype(BF)
    for b in range(8):
        cols = slice(b * BLK, (b + 1) * BLK)
        mix = jnp.dot(pooled[...], outfull[:, cols], preferred_element_type=F32)
        v = (xall2[b].astype(F32) + mix * sall[b, 0:1, 0:256]).astype(BF)
        ambuf[b] = v
        nbuf[:, cols] = norm_block(b, ambuf, gain2, b == 0)
    finish_norm()

    for j in range(6):
        hidden(j)

    def products2(k):
        chip = (x + (0, 1, 2, -1)[k] + NX) % NX
        res = down(chip, slice(0, 2 * BLK))
        snd2[k] = res[:, OTHER].astype(BF)
        second.pair(k).start()
        mine[k] = res[:, OWN]

    def both(k):
        second.pair(k).wait_recv()
        return mine[k] + pre2[k].astype(F32)

    products2(2)
    products2(1)
    products2(3)
    second.far(both(2))
    second.near_right(both(1))
    products2(0)
    second.near_left(both(3))
    tot[0] = both(0)
    for q in SEQS:
        second.through(q)
    for q in SEQS:
        rows = pl.ds(SEQ * q, SEQ)
        out[rows, :] = (ambuf[t, rows, :].astype(F32) + 0.5 * (second.total(q) * dsc[...])).astype(BF)

    for ref, k in ((pall.at[0, pl.ds(0, 31 * 64), :], 0), (gbuf.at[pl.ds(0, 124 * 16), :], 1), (dbuf.at[pl.ds(0, 62 * 176), :], 2)):
        pltpu.make_async_remote_copy(
            src_ref=ref, dst_ref=ref, send_sem=psend.at[k], recv_sem=precv.at[0, 0], device_id={"fs": neighbour[0], "tp": t}
        ).wait_send()
    for ring in (ag1, sag, pag, gather):
        ring.done()
    first.done()
    second.done()


def body(
    stream, gain_first, gain_mixer, gain_second, gate_weight, gate_scale, up_weight, up_scale,
    down_weight, down_scale, pool_in_weight, pool_in_scale, pool_out_weight, pool_out_scale,
):
    def line(v):
        return v.reshape(1, -1)

    operands = (
        stream, line(gain_first), line(gain_mixer), line(gain_second), gate_weight, gate_scale, up_weight,
        up_scale, down_weight.T, line(down_scale), pool_in_weight, line(pool_in_scale), pool_out_weight,
        line(pool_out_scale),
    )
    vmem = pl.BlockSpec(memory_space=pltpu.VMEM)
    V = pltpu.VMEM
    sem = pltpu.SemaphoreType.DMA
    exchange = [V((4, ROWS, BLK), BF), V((4, ROWS, BLK), BF), V((3, ROWS, BLK), BF), V((3, ROWS, BLK), BF)]
    ring_sems = [sem((2,)), sem((14,))]
    return pl.pallas_call(
        kernel,
        out_shape=jax.ShapeDtypeStruct((ROWS, BLK), BF),
        in_specs=[pl.BlockSpec(memory_space=pltpu.HBM)] * 14,
        out_specs=vmem,
        scratch_shapes=[
            V((D, GUW), BF),
            V((32 * DH, 128), BF),
            V((NX, 768, 2 * BLK), BF),
            V((8, D, 128), BF),
            V((8, 16, 384), F32),
            V((D, 512), BF),
            V((512, D), BF),
            V((8, ROWS, BLK), BF),
            V((8, ROWS, BLK), BF),
            V((ROWS, D), BF),
            V((8, ROWS, BLK), BF),
            V((ROWS, 768), BF),
            V((ROWS, 128), F32),
            V((ROWS, 128), F32),
            V((ROWS, 512), F32),
            V((ROWS, 512), BF),
            *exchange,
            *exchange,
            V((4, ROWS, BLK), F32),
            V((4, ROWS, BLK), F32),
            V((1, FB), F32), V((1, FB), F32),
            sem((3,)), sem((7, 32)),
            *ring_sems, sem((2,)), sem((42,)), *ring_sems, *ring_sems,
            sem((2,)), sem((22,)), sem((2,)), sem((22,)),
            V((1, D), F32), V((1, D), F32), V((1, D), F32), V((64, FB), F32), V((FB,), F32), V((64, FB), F32), V((FB,), F32),
            V((64, FB), F32), V((1, BLK), F32), V((64, 64), F32), V((1, 64), F32), V((64, 64), F32), V((1, BLK), F32),
            sem((14,)),
        ],
        compiler_params=pltpu.CompilerParams(
            collective_id=0, has_side_effects=True, vmem_limit_bytes=42 * 1024 * 1024
        ),
    )(*(pltpu.with_memory_space_constraint(v, pltpu.HBM) for v in operands))


def solution(mesh):
    placed = (
        P("fs", "tp"), P(), P(), P(), P("fs", "tp"), P("tp"), P("fs", "tp"), P("tp"), P("tp", "fs"), P("tp"),
        P("fs", "tp"), P("tp"), P("tp", "fs"), P("tp"),
    )
    return jax.shard_map(body, mesh=mesh, in_specs=placed, out_specs=P("fs", "tp"), check_vma=False)
```

```python
import random

import jax
import jax.numpy as jnp
from jax import lax
from jax.experimental import pallas as pl
from jax.experimental.pallas import tpu as pltpu
from jax.sharding import PartitionSpec as P

SEQ = 128
EPS = 1e-06
WINDOWS = (2, 4, 8, 16)
NZ, NY, NX = 8, 4, 4
ROWS = 384
HALF = ROWS // 2
D = 2048
BLK = 256
FB = 704
GUW = 2 * FB
DH = FB // 2
BF = jnp.bfloat16
F32 = jnp.float32

SIZES = (0.36, 1, 1, 1, 1, 1, 1)
RANKS = (-1, 0, 0, 0, 0, 1, 1)
PIECES_G = (1, 2, 3, 4)
PIECES_D = (5, 6)
PLAN = (4.0, 10186, 1.0)
G_LATE, D_LATE = 1.0, 0.5


def moved(o, d):
    z, y = o
    if d == 0:
        return z, (y + 1) % NY
    if d == 1:
        return z, (y - 1) % NY
    return (z + (1 if d == 2 else -1)) % NZ, y


def broadcast_plan(lag=PLAN[0], seed=PLAN[1], noise=PLAN[2]):
    rng = random.Random(seed)
    count = len(SIZES)
    has = [{(0, 0): 0.0} for _ in range(count)]
    free = [0.0] * 4
    plan = []
    while len(plan) < count * (NZ * NY - 1):
        best = None
        for d in range(4):
            found = []
            for s in range(count):
                for o, t in has[s].items():
                    q = moved(o, d)
                    if q not in has[s]:
                        found.append((max(free[d], t), s, o, q))
            if found:
                first = min(c[0] for c in found)
                if best is None or first < best[0]:
                    best = (first, d, [c for c in found if c[0] <= first + 1e-9])
        _, d, found = best

        def key(c):
            onward = sum(moved(c[3], e) not in has[c[1]] for e in range(4))
            return RANKS[c[1]] * 1.5 - noise * rng.random() * 4 - onward * 0.5 + len(has[c[1]]) * 0.02

        start, s, o, q = min(found, key=key)
        has[s][q] = start + SIZES[s] + lag
        free[d] = start + SIZES[s]
        plan.append((start, d, s, o))
    return plan, has


def kernel(
    *refs,
):
    hbm, out, rest = refs[:14], refs[14], refs[15:]
    (
        gbuf, dbuf, dfull, pall, sall, infull, outfull, xall1, xall2, nbuf, ambuf, hid, ssacc, rst, pacc, pooled,
        snd1, pre1, sr1, rr1, snd2, pre2, sr2, rr2, mine, tot,
        gsc, usc, psend, precv, a1s, a1r, a2s, a2r, pas, par, sas, sar, r1s, r1r, r2s, r2r,
        gain1, gainm, gain2, gw, gsc1, uw, usc1, dw, dsc, iw, isc, ow, osc, insem,
    ) = rest
    f, t = lax.axis_index("fs"), lax.axis_index("tp")
    z, y = f // NY, f % NY
    x, c = t // 2, t % 2
    oc = 1 - c

    def at_f(dz, dy):
        return ((z + dz + NZ) % NZ) * NY + (y + dy + NY) % NY

    def at_t(dx, core):
        return ((x + dx + NX) % NX) * 2 + core

    inputs = [
        pltpu.make_async_copy(src, dst, insem.at[i])
        for i, (src, dst) in enumerate(
            zip(hbm, (xall1.at[t], gain1, gainm, gain2, gw, gsc1, uw, usc1, dw, dsc, iw, isc, ow, osc))
        )
    ]
    for i in (10, 12, 4, 6, 8, 0, 1, 2, 3, 5, 7, 9, 11, 13):
        inputs[i].start()

    neighbour = [at_f(0, 1), at_f(0, -1), at_f(1, 0), at_f(-1, 0)]
    right, left, twin = at_t(1, c), at_t(-1, c), at_t(0, oc)

    barrier = pltpu.get_barrier_semaphore()
    for nf in neighbour:
        pl.semaphore_signal(barrier, inc=1, device_id={"fs": nf, "tp": t})
    for nt in (right, left, twin):
        pl.semaphore_signal(barrier, inc=1, device_id={"fs": f, "tp": nt})

    prow = pl.ds(pl.multiple_of(f * 64, 64), 64)
    inputs[10].wait()
    inputs[12].wait()
    pall[t, prow, :] = jnp.concatenate([iw[...], ow[...]], axis=1).astype(BF)
    inputs[4].wait()
    inputs[6].wait()
    for j in range(5):
        gbuf[prow, 256 * j : 256 * j + 128] = gw[:, 128 * j : 128 * j + 128].astype(BF)
        gbuf[prow, 256 * j + 128 : 256 * j + 256] = uw[:, 128 * j : 128 * j + 128].astype(BF)
    gbuf[prow, 1280:1408] = jnp.concatenate([gw[:, 640:704], uw[:, 640:704]], axis=1).astype(BF)
    pl.semaphore_wait(barrier, 7)

    def pack_rest():
        for i in (8, 0, 1, 2, 3, 5, 7, 9, 11, 13):
            inputs[i].wait()
        down_rows = jnp.transpose(dw[...])
        dbuf[pl.ds(pl.multiple_of(f * DH, 32), DH), :] = jnp.concatenate(
            [down_rows[0:DH, :], down_rows[DH:FB, :]], axis=1
        ).astype(BF)
        sall[t] = jnp.concatenate(
            [jnp.broadcast_to(osc[...], (16, 256)), jnp.broadcast_to(isc[...], (16, 64)), jnp.zeros((16, 64), F32)], axis=1
        )
        gsc[...] = gsc1[...].reshape(1, FB)
        usc[...] = usc1[...].reshape(1, FB)

    def piece(s, owner):
        if s == 0:
            return pall.at[t, pl.ds(pl.multiple_of(owner * 64, 64), 64), :]
        if s in PIECES_G:
            return gbuf.at[pl.ds(pl.multiple_of(owner * 64 + 16 * (s - 1), 16), 16), :]
        return dbuf.at[pl.ds(pl.multiple_of(owner * DH + 176 * (s - 5), 16), 176), :]

    def owner_of(o):
        return at_f(-o[0], -o[1])

    arrived = set()

    def ensure(s, o):
        if o == (0, 0) or (s, o) in arrived:
            return
        arrived.add((s, o))
        ref = piece(s, owner_of(o))
        pltpu.make_async_remote_copy(
            src_ref=ref, dst_ref=ref, send_sem=psend.at[0], recv_sem=precv.at[s, o[0] * NY + o[1]],
            device_id={"fs": neighbour[0], "tp": t},
        ).wait_recv()

    def send_piece(d, s, o):
        ensure(s, o)
        q = moved(o, d)
        ref = piece(s, owner_of(o))
        pltpu.make_async_remote_copy(
            src_ref=ref, dst_ref=ref, send_sem=psend.at[0 if s == 0 else 1 if s in PIECES_G else 2],
            recv_sem=precv.at[s, q[0] * NY + q[1]], device_id={"fs": neighbour[d], "tp": t},
        ).start()

    class Ring:
        def __init__(self, part, whole, ssem, rsem, base=0):
            self.part, self.whole, self.ssem, self.rsem, self.base = part, whole, ssem, rsem, base

        def copy(self, ref, to, rs):
            return pltpu.make_async_remote_copy(
                src_ref=ref, dst_ref=ref, send_sem=self.ssem.at[1 if rs >= 6 else 0], recv_sem=self.rsem.at[self.base + rs],
                device_id={"fs": f, "tp": to},
            )

        def start(self):
            me = t
            self.copy(self.part(me, 0), right, 0).start()
            self.copy(self.part(me, 1), left, 3).start()
            self.copy(self.part(me, 1), right, 1).start()
            self.copy(self.part(me, 0), left, 2).start()
            self.copy(self.part(me, 0), twin, 6).start()
            self.copy(self.part(me, 1), twin, 7).start()

        def block(self, k, core):
            return at_t((-1, -1, 1, 1, 2, 2, 0, 0)[k], core), k % 2

        def got(self, k, share=True):
            ref = self.part(*self.block(k, c))
            self.copy(ref, twin, k).wait_recv()
            if k == 0:
                self.copy(ref, right, 4).start()
            if k == 3:
                self.copy(ref, left, 5).start()
            if share:
                self.copy(ref, twin, 8 + k).start()

        def got_twin(self, k):
            ref = self.part(*self.block(k, oc))
            self.copy(ref, twin, 8 + k if k < 6 else k).wait_recv()

        def done(self):
            pltpu.make_async_remote_copy(
                src_ref=self.whole(3), dst_ref=self.whole(3), send_sem=self.ssem.at[0], recv_sem=self.rsem.at[0],
                device_id={"fs": f, "tp": twin},
            ).wait_send()
            pltpu.make_async_remote_copy(
                src_ref=self.whole(4), dst_ref=self.whole(4), send_sem=self.ssem.at[1], recv_sem=self.rsem.at[0],
                device_id={"fs": f, "tp": twin},
            ).wait_send()

    def halves(buf, size):
        return (
            lambda b, h: buf.at[b, pl.ds(h * (size // 2), size // 2), :],
            lambda n: buf.at[pl.ds(0, n)],
        )

    ag1 = Ring(*halves(xall1, ROWS), a1s, a1r)
    pag = Ring(*halves(pall, D), pas, par)
    sag = Ring(*halves(sall, 16), sas, sar)
    sag.part = lambda b, h: sall.at[b, pl.ds(h * 8, 8), :]

    def norm_block(b, src, gain, first):
        v = src[b].astype(F32)
        sq = v * v
        sq = sq[:, :128] + sq[:, 128:]
        ssacc[...] = sq if first else ssacc[...] + sq
        return (v * gain[:, b * BLK : (b + 1) * BLK]).astype(BF)

    def finish_norm():
        mean = jnp.sum(ssacc[...], axis=1, keepdims=True) * (1.0 / D)
        rst[...] = jnp.broadcast_to(lax.rsqrt(mean + EPS), (ROWS, 128))

    def norm1(b):
        nbuf[:, b * BLK : (b + 1) * BLK] = norm_block(b, xall1, gain1, b == 0)

    def hidden(j, at=0, size=ROWS):
        rows = slice(at, at + size)
        r = rst[rows, :]
        if j < 5:
            acc = jnp.dot(nbuf[rows, :], gbuf[:, 256 * j : 256 * j + 256], preferred_element_type=F32)
            g = acc[:, :128] * r * gsc[:, 128 * j : 128 * j + 128]
            u = acc[:, 128:] * r * usc[:, 128 * j : 128 * j + 128]
            hid[rows, 128 * j : 128 * j + 128] = (g / (1.0 + jnp.exp(-g)) * u).astype(BF)
        else:
            acc = jnp.dot(nbuf[rows, :], gbuf[:, 1280:1408], preferred_element_type=F32)
            scale = jnp.concatenate([gsc[:, 640:704], usc[:, 640:704]], axis=1)
            v = acc * r * scale
            u = pltpu.roll(v, 64, 1)
            h = v / (1.0 + jnp.exp(-v)) * u
            lane = lax.broadcasted_iota(jnp.int32, h.shape, 1)
            hid[rows, 640:768] = jnp.where(lane < 64, h, 0.0).astype(BF)

    def unpack_down(b):
        side = (b + c) % 2
        for pair in range(2):
            one = dbuf[pl.ds(pl.multiple_of((4 * b + 2 * pair) * DH, 32), DH), :]
            two = dbuf[pl.ds(pl.multiple_of((4 * b + 2 * pair + 1) * DH, 32), DH), :]
            cols = pl.ds(pl.multiple_of(side * BLK + 128 * pair, 128), 128)
            dfull[b // 2, 0:DH, cols] = jnp.concatenate([one[:, :64], two[:, :64]], axis=1)
            dfull[b // 2, DH:FB, cols] = jnp.concatenate([one[:, 64:], two[:, 64:]], axis=1)

    def unpack_in(k):
        rows = pl.ds(256 * k, 256)
        for i in range(NX):
            infull[rows, 128 * i : 128 * i + 128] = jnp.concatenate(
                [pall[2 * i, rows, :][:, :64], pall[2 * i + 1, rows, :][:, :64]], axis=1
            )

    def unpack_out(b):
        for i in range(16):
            outfull[64 * b : 64 * b + 64, 128 * i : 128 * i + 128] = jnp.concatenate(
                [pall[b, 128 * i : 128 * i + 64, :][:, 64:], pall[b, 128 * i + 64 : 128 * i + 128, :][:, 64:]], axis=1
            )

    def down(chip, cols):
        return jnp.dot(hid[...], dfull[chip, :, cols], preferred_element_type=F32)

    OWN, OTHER = slice(0, BLK), slice(BLK, 2 * BLK)

    SEQS = range(ROWS // SEQ)

    class Sum:
        def __init__(self, snd, pre, sr, rr, ss, rs):
            self.snd, self.pre, self.sr, self.rr, self.ss, self.rs = snd, pre, sr, rr, ss, rs

        def pair(self, k):
            return pltpu.make_async_remote_copy(
                src_ref=self.snd.at[k], dst_ref=self.pre.at[k], send_sem=self.ss.at[0], recv_sem=self.rs.at[k],
                device_id={"fs": f, "tp": twin},
            )

        def half(self, q, h):
            return pl.ds(SEQ * q + h * (SEQ // 2), SEQ // 2)

        def hop(self, q, src, slot, h, sem, to):
            rows = self.half(q, h)
            return pltpu.make_async_remote_copy(
                src_ref=self.sr.at[src, rows, :], dst_ref=self.rr.at[slot, rows, :], send_sem=self.ss.at[1],
                recv_sem=self.rs.at[4 + 6 * q + sem], device_id={"fs": f, "tp": to},
            )

        def far(self, total):
            self.sr[2] = total.astype(BF)
            for q in SEQS:
                self.hop(q, 2, 2, 0, 0, right).start()
                self.hop(q, 2, 2, 1, 1, left).start()

        def near_right(self, total):
            tot[1] = total
            for q in SEQS:
                rows = self.half(q, 1)
                self.sr[1, rows, :] = tot[1, rows, :].astype(BF)
                self.hop(q, 1, 0, 1, 2, right).start()

        def near_left(self, total):
            tot[3] = total
            for q in SEQS:
                rows = self.half(q, 0)
                self.sr[0, rows, :] = tot[3, rows, :].astype(BF)
                self.hop(q, 0, 1, 0, 3, left).start()

        def through(self, q):
            rows = self.half(q, 0)
            self.hop(q, 2, 2, 0, 0, right).wait_recv()
            self.sr[1, rows, :] = (tot[1, rows, :] + self.rr[2, rows, :].astype(F32)).astype(BF)
            self.hop(q, 1, 0, 0, 4, right).start()
            rows = self.half(q, 1)
            self.hop(q, 2, 2, 1, 1, left).wait_recv()
            self.sr[0, rows, :] = (tot[3, rows, :] + self.rr[2, rows, :].astype(F32)).astype(BF)
            self.hop(q, 0, 1, 1, 5, left).start()

        def total(self, q):
            self.hop(q, 1, 0, 1, 2, right).wait_recv()
            self.hop(q, 0, 1, 0, 3, left).wait_recv()
            self.hop(q, 1, 0, 0, 4, right).wait_recv()
            self.hop(q, 0, 1, 1, 5, left).wait_recv()
            rows = pl.ds(SEQ * q, SEQ)
            return tot[0, rows, :] + self.rr[0, rows, :].astype(F32) + self.rr[1, rows, :].astype(F32)

        def done(self):
            for ref, k in ((self.snd.at[pl.ds(0, 4)], 0), (self.sr.at[pl.ds(0, 3)], 1)):
                pltpu.make_async_remote_copy(
                    src_ref=ref, dst_ref=ref, send_sem=self.ss.at[k], recv_sem=self.rs.at[0],
                    device_id={"fs": f, "tp": twin},
                ).wait_send()

    first = Sum(snd1, pre1, sr1, rr1, r1s, r1r)
    second = Sum(snd2, pre2, sr2, rr2, r2s, r2r)

    plan, has = broadcast_plan()
    events = []

    def when(time, fn):
        events.append((time, len(events), fn))

    for start, d, s, o in plan:
        when(start, lambda d=d, s=s, o=o: send_piece(d, s, o))

    first_down = min(start for start, _, s, _ in plan if s in PIECES_D)
    when(min(0.4, first_down - 1e-3), pack_rest)
    when(1.5, ag1.start)
    when(1.6, sag.start)
    for k, time in ((0, 5.5), (3, 5.5), (1, 8.5), (2, 8.5), (4, 11.0), (5, 11.0)):
        when(time, lambda k=k: ag1.got(k))
        when(time + 0.01, lambda k=k: sag.got(k))

    def twin1():
        for k in range(8):
            ag1.got_twin(k)
            sag.got_twin(k)

    when(13.0, twin1)
    for b in range(8):
        when(13.2 + 0.6 * b, lambda b=b: norm1(b))
    when(18.2, finish_norm)

    p_done = max(has[0].values())

    def pool_ring():
        for o in has[0]:
            ensure(0, o)
        pag.start()

    when(p_done, pool_ring)
    for k, time in ((0, 8.5), (3, 8.5), (1, 15.0), (2, 15.0), (4, 22.5), (5, 22.5)):
        when(p_done + time, lambda k=k: pag.got(k))

    def twin_pool():
        for k in range(8):
            pag.got_twin(k)


    g_done = max(max(has[s].values()) for s in PIECES_G)

    def gates():
        for s in PIECES_G:
            for o in has[s]:
                ensure(s, o)

    when(g_done + G_LATE, gates)

    def hidden_part(js):
        for j in js:
            hidden(j)

    when(g_done + G_LATE + 0.1, lambda: hidden_part((0, 1, 2)))
    when(g_done + G_LATE + 1.9, lambda: hidden_part((3, 4, 5)))

    def plane(oz):
        for s in PIECES_D:
            for oy in range(NY):
                ensure(s, (oz, oy))
        unpack_down((z - oz + NZ) % NZ)

    def clear_down():
        dfull[:, FB:768, :] = jnp.zeros((NX, 768 - FB, 2 * BLK), BF)

    when(0.5, clear_down)
    ready = {oz: max(has[s][oz, oy] for s in PIECES_D for oy in range(NY)) for oz in range(NZ)}
    even, odd = (sorted(range(e, NZ, 2), key=lambda oz: ready[oz]) for e in (0, 1))
    turn = (z + c) % 2

    def products(i):
        one, two = (z - even[i] + NZ) % NZ, (z - odd[i] + NZ) % NZ
        for_twin = one * turn + two * (1 - turn)
        own = two * turn + one * (1 - turn)
        theirs, ours = down(for_twin // 2, OTHER), down(own // 2, OWN)
        snd1[i] = theirs.astype(BF)
        mine[i] = ours
        first.pair(i).start()

    def combine(i):
        one, two = (z - even[i] + NZ) % NZ, (z - odd[i] + NZ) % NZ
        own = two * turn + one * (1 - turn)
        away = (own // 2 - x + NX) % NX
        first.pair(i).wait_recv()
        mine[i] = mine[i] + pre1[i].astype(F32)

        @pl.when(away == 2)
        def _():
            first.far(mine[i])

        @pl.when(away == 1)
        def _():
            first.near_right(mine[i])

        @pl.when(away == 3)
        def _():
            first.near_left(mine[i])

        @pl.when(away == 0)
        def _():
            tot[0] = mine[i]

    hid_done = g_done + G_LATE + 3.6
    for oz in range(NZ):
        when(ready[oz] + D_LATE, lambda oz=oz: plane(oz))
    for i in range(4):
        at = max(hid_done + 1.0 * i, max(ready[even[i]], ready[odd[i]]) + D_LATE + 0.01)
        when(at, lambda i=i: products(i))
        when(at + 1.6, lambda i=i: combine(i))

    def pool_weights():
        twin_pool()
        for b in range(8):
            unpack_out(b)

    when(at + 0.2, pool_weights)

    for _, _, fn in sorted(events, key=lambda e: e[:2]):
        fn()

    for q in SEQS:
        first.through(q)
    gathers = []
    for q in SEQS:
        gather = Ring(
            lambda b, h, q=q: xall2.at[b, pl.ds(SEQ * q + h * (SEQ // 2), SEQ // 2), :],
            lambda n: xall2.at[pl.ds(0, n)], a2s, a2r, 14 * q,
        )
        gathers.append(gather)
        rows = pl.ds(SEQ * q, SEQ)
        xall2[t, rows, :] = (xall1[t, rows, :].astype(F32) + 0.5 * (first.total(q) * dsc[...])).astype(BF)
        gather.start()

    def enter(b, start=False):
        v = xall2[b].astype(F32)
        sq = v * v
        sq = sq[:, :128] + sq[:, 128:]
        at = pl.multiple_of(b * BLK, BLK)
        w = (v * gainm[:, pl.ds(at, BLK)]).astype(BF)
        part = jnp.dot(w, infull[pl.ds(at, BLK), :], preferred_element_type=F32)
        ssacc[...] = sq if start else ssacc[...] + sq
        pacc[...] = part if start else pacc[...] + part

    for b in range(8):
        unpack_in(b)
    enter(t, True)
    for q in SEQS:
        for k in (0, 3):
            gathers[q].got(k)
    for q in SEQS:
        gathers[q].got_twin(6)
        gathers[q].got_twin(7)
    enter(twin)
    for q in SEQS:
        for k in (1, 2):
            gathers[q].got(k)
    enter(left)
    enter(right)
    for q in SEQS:
        for k in (0, 1, 2, 3):
            gathers[q].got_twin(k)
    enter(at_t(-1, oc))
    enter(at_t(1, oc))
    for q in SEQS:
        for k in (4, 5):
            gathers[q].got(k)
    enter(at_t(2, c))
    for q in SEQS:
        for k in (4, 5):
            gathers[q].got_twin(k)
    enter(at_t(2, oc))
    finish_norm()
    row = lax.broadcasted_iota(jnp.int32, (SEQ, SEQ), 0)
    col = lax.broadcasted_iota(jnp.int32, (SEQ, SEQ), 1)
    for g, window in enumerate(WINDOWS):
        low = jnp.maximum(row - window // 2, 0)
        high = jnp.minimum(row + window - window // 2, SEQ)
        band = jnp.where((col >= low) & (col < high), 1.0, 0.0).astype(BF)
        count = (high - low).astype(F32)
        scale = jnp.concatenate([sall[2 * g, 0:1, 256:320], sall[2 * g + 1, 0:1, 256:320]], axis=1)
        cols = slice(128 * g, 128 * g + 128)
        value = (pacc[:, cols] * rst[...] * scale).astype(BF)
        side = jnp.concatenate([value[SEQ * q : SEQ * q + SEQ] for q in SEQS], axis=1)
        whole = jnp.dot(band, side, preferred_element_type=F32)
        for q in SEQS:
            rows = slice(SEQ * q, SEQ * q + SEQ)
            mean = whole[:, SEQ * q : SEQ * q + SEQ] / count
            pooled[rows, cols] = (mean - value[rows].astype(F32)).astype(BF)
    for b in range(8):
        cols = slice(b * BLK, (b + 1) * BLK)
        mix = jnp.dot(pooled[...], outfull[:, cols], preferred_element_type=F32)
        v = (xall2[b].astype(F32) + mix * sall[b, 0:1, 0:256]).astype(BF)
        ambuf[b] = v
        nbuf[:, cols] = norm_block(b, ambuf, gain2, b == 0)
    finish_norm()

    for j in range(6):
        hidden(j)

    def products2(k):
        chip = (x + (0, 1, 2, -1)[k] + NX) % NX
        res = down(chip, slice(0, 2 * BLK))
        snd2[k] = res[:, OTHER].astype(BF)
        second.pair(k).start()
        mine[k] = res[:, OWN]

    def both(k):
        second.pair(k).wait_recv()
        return mine[k] + pre2[k].astype(F32)

    products2(2)
    products2(1)
    products2(3)
    second.far(both(2))
    second.near_right(both(1))
    products2(0)
    second.near_left(both(3))
    tot[0] = both(0)
    for q in SEQS:
        second.through(q)
    for q in SEQS:
        rows = pl.ds(SEQ * q, SEQ)
        out[rows, :] = (ambuf[t, rows, :].astype(F32) + 0.5 * (second.total(q) * dsc[...])).astype(BF)

    for ref, k in ((pall.at[0, pl.ds(0, 31 * 64), :], 0), (gbuf.at[pl.ds(0, 124 * 16), :], 1), (dbuf.at[pl.ds(0, 62 * 176), :], 2)):
        pltpu.make_async_remote_copy(
            src_ref=ref, dst_ref=ref, send_sem=psend.at[k], recv_sem=precv.at[0, 0], device_id={"fs": neighbour[0], "tp": t}
        ).wait_send()
    for ring in (ag1, sag, pag, gather):
        ring.done()
    first.done()
    second.done()


def body(
    stream, gain_first, gain_mixer, gain_second, gate_weight, gate_scale, up_weight, up_scale,
    down_weight, down_scale, pool_in_weight, pool_in_scale, pool_out_weight, pool_out_scale,
):
    def line(v):
        return v.reshape(1, -1)

    operands = (
        stream, line(gain_first), line(gain_mixer), line(gain_second), gate_weight, gate_scale, up_weight,
        up_scale, down_weight.T, line(down_scale), pool_in_weight, line(pool_in_scale), pool_out_weight,
        line(pool_out_scale),
    )
    vmem = pl.BlockSpec(memory_space=pltpu.VMEM)
    V = pltpu.VMEM
    sem = pltpu.SemaphoreType.DMA
    exchange = [V((4, ROWS, BLK), BF), V((4, ROWS, BLK), BF), V((3, ROWS, BLK), BF), V((3, ROWS, BLK), BF)]
    ring_sems = [sem((2,)), sem((14,))]
    return pl.pallas_call(
        kernel,
        out_shape=jax.ShapeDtypeStruct((ROWS, BLK), BF),
        in_specs=[pl.BlockSpec(memory_space=pltpu.HBM)] * 14,
        out_specs=vmem,
        scratch_shapes=[
            V((D, GUW), BF),
            V((32 * DH, 128), BF),
            V((NX, 768, 2 * BLK), BF),
            V((8, D, 128), BF),
            V((8, 16, 384), F32),
            V((D, 512), BF),
            V((512, D), BF),
            V((8, ROWS, BLK), BF),
            V((8, ROWS, BLK), BF),
            V((ROWS, D), BF),
            V((8, ROWS, BLK), BF),
            V((ROWS, 768), BF),
            V((ROWS, 128), F32),
            V((ROWS, 128), F32),
            V((ROWS, 512), F32),
            V((ROWS, 512), BF),
            *exchange,
            *exchange,
            V((4, ROWS, BLK), F32),
            V((4, ROWS, BLK), F32),
            V((1, FB), F32), V((1, FB), F32),
            sem((3,)), sem((7, 32)),
            *ring_sems, sem((2,)), sem((42,)), *ring_sems, *ring_sems,
            sem((2,)), sem((22,)), sem((2,)), sem((22,)),
            V((1, D), F32), V((1, D), F32), V((1, D), F32), V((64, FB), F32), V((FB,), F32), V((64, FB), F32), V((FB,), F32),
            V((64, FB), F32), V((1, BLK), F32), V((64, 64), F32), V((1, 64), F32), V((64, 64), F32), V((1, BLK), F32),
            sem((14,)),
        ],
        compiler_params=pltpu.CompilerParams(
            collective_id=0, has_side_effects=True, vmem_limit_bytes=42 * 1024 * 1024
        ),
    )(*(pltpu.with_memory_space_constraint(v, pltpu.HBM) for v in operands))


def solution(mesh):
    placed = (
        P("fs", "tp"), P(), P(), P(), P("fs", "tp"), P("tp"), P("fs", "tp"), P("tp"), P("tp", "fs"), P("tp"),
        P("fs", "tp"), P("tp"), P("tp", "fs"), P("tp"),
    )
    return jax.shard_map(body, mesh=mesh, in_specs=placed, out_specs=P("fs", "tp"), check_vma=False)
```
